32 devices in a mesh: sp: 8 (over z, x), tp: 4 (over y, core).
Axes of the slice: x: 2, y: 2, z: 4, core: 2. Of those that a mesh axis runs over, the one named last changes fastest.
Arguments:
- residual: bfloat16 [4096, 2048], P(('sp', 'tp')), may hold values from -6 to 6
- query_small: bfloat16 [4096, 8, 128], P('sp', 'tp'), may hold values from -120 to 120
- key_small: bfloat16 [4096, 8, 128], P('sp', 'tp'), may hold values from -6 to 6
- value_small: bfloat16 [4096, 8, 128], P('sp', 'tp'), may hold values from -6 to 6
- query_large: bfloat16 [4096, 8, 256], P('sp', 'tp'), may hold values from -120 to 120
- key_large: bfloat16 [4096, 8, 256], P('sp', 'tp'), may hold values from -6 to 6
- value_large: bfloat16 [4096, 8, 128], P('sp', 'tp'), may hold values from -6 to 6
- lambda_small: float32 [8], P('tp'), may hold values from 0.3 to 0.8
- lambda_large: float32 [8], P('tp'), may hold values from 0.3 to 0.8
- head_gain: float32 [128], replicated, may hold values from 0.1 to 1.9
- output_small: bfloat16 [1024, 2048], P('tp'), may hold values from -0.125 to 0.125
- output_large: bfloat16 [1024, 2048], P('tp'), may hold values from -0.125 to 0.125
- norm_gain: float32 [2048], replicated, may hold values from 0.1 to 1.9
- gate_weight: bfloat16 [2048, 5632], P('sp', 'tp'), may hold values from -0.125 to 0.125
- up_weight: bfloat16 [2048, 5632], P('sp', 'tp'), may hold values from -0.125 to 0.125
- down_weight: bfloat16 [5632, 2048], P('tp', 'sp'), may hold values from -0.3125 to 0.3125
Outputs:
- block_output: bfloat16 [4096, 2048], P(('sp', 'tp'))
The draws below stay inside these ranges and needn't reach their ends.
All inputs are finite; a program needn't handle non-finite values.
Results may differ from the reference program's by a relative error of at most 0.015.
Values may be sent and summed in bfloat16 or wider, within the bound.
A program may use at most 128 MiB of HBM per device.

```python
import math
import jax
import jax.numpy as jnp
from jax import lax

D = 2048
HA = 8
HB = 8
KA = 64
KB = 128
VD = 128
FF = 5632
SEQ = 4096


def draw_pair(key, head_count, width, salt):
    base = jax.random.fold_in(key, salt)
    key_draw, query_draw = jax.random.split(base, 2)
    key_rows = jnp.clip(1.3 * jax.random.normal(key_draw, (SEQ, head_count, width), jnp.float32), -6.0, 6.0)
    query_rows = jnp.clip(1.3 * jax.random.normal(query_draw, (SEQ, head_count, width), jnp.float32), -6.0, 6.0)
    return (query_rows, key_rows)


def draw_query_small(key, part):
    return draw_pair(key, HA, 2 * KA, 11)[0].astype(jnp.bfloat16)


def draw_key_small(key, part):
    return draw_pair(key, HA, 2 * KA, 11)[1].astype(jnp.bfloat16)


def draw_query_large(key, part):
    return draw_pair(key, HB, 2 * KB, 23)[0].astype(jnp.bfloat16)


def draw_key_large(key, part):
    return draw_pair(key, HB, 2 * KB, 23)[1].astype(jnp.bfloat16)


def block_levels(key, shape, shards, least, largest):
    def one(position, blocks):
        heights = jax.random.uniform(jax.random.fold_in(jax.random.fold_in(key, 6), position), (blocks,), jnp.float32, least / len(shards), largest / len(shards))
        return jnp.repeat(jnp.exp(heights), shape[position] // blocks).reshape((-1,) + (1,) * (len(shape) - position - 1))

    factor_of = one(*shards[0])
    for cut in shards[1:]:
        factor_of = factor_of * one(*cut)
    return factor_of


def scatter_about(key, shape, scale, bound, shards=(), kind=jnp.bfloat16):
    values = jax.random.normal(key, shape, jnp.float32) * scale
    if len(shards) > 0:
        values = block_levels(key, shape, shards, -0.22, 0.18) * values
    return jnp.clip(values, min=-bound, max=bound).astype(kind)


def setup_inputs(seed: int = 0) -> dict:
    key_list = jax.random.split(jax.random.key(seed), 17)
    return {
        "residual": scatter_about(key_list[0], (SEQ, D), 1.0, 6.0, ((0, 32),)),
        "query_small": draw_query_small(jax.random.fold_in(key_list[16], 71), 0),
        "key_small": draw_key_small(jax.random.fold_in(key_list[16], 71), 0),
        "value_small": scatter_about(key_list[3], (SEQ, HA, VD), 1.0, 6.0, ((0, 8), (1, 4))),
        "query_large": draw_query_large(jax.random.fold_in(key_list[16], 71), 0),
        "key_large": draw_key_large(jax.random.fold_in(key_list[16], 71), 0),
        "value_large": scatter_about(key_list[6], (SEQ, HB, VD), 1.0, 6.0, ((0, 8), (1, 4))),
        "lambda_small": jnp.clip(0.3 + 0.5 * jax.random.uniform(key_list[7], (HA,), jnp.float32) ** block_levels(key_list[7], (HA,), ((0, 4),), -0.2, 0.2), 0.3, 0.8),
        "lambda_large": jnp.clip(0.3 + 0.5 * jax.random.uniform(key_list[8], (HB,), jnp.float32) ** block_levels(key_list[8], (HB,), ((0, 4),), -0.2, 0.2), 0.3, 0.8),
        "head_gain": jnp.clip(1.0 + 0.18 * jax.random.normal(key_list[9], (VD,), jnp.float32), 0.1, 1.9),
        "output_small": scatter_about(key_list[10], (HA * VD, D), ((HA + HB) * VD) ** -0.5, 0.125, ((0, 4),)),
        "output_large": scatter_about(key_list[11], (HB * VD, D), ((HA + HB) * VD) ** -0.5, 0.125, ((0, 4),)),
        "norm_gain": jnp.clip(1.0 + 0.18 * jax.random.normal(key_list[12], (D,), jnp.float32), 0.1, 1.9),
        "gate_weight": scatter_about(key_list[13], (D, FF), D ** -0.5, 0.125, ((0, 8), (1, 4))),
        "up_weight": scatter_about(key_list[14], (D, FF), D ** -0.5, 0.125, ((0, 8), (1, 4))),
        "down_weight": scatter_about(key_list[15], (FF, D), (FF // 16) ** -0.5, 0.3125, ((0, 4), (1, 8))),
    }


residual_scale = 8.0 ** 0.25
branch_scale = 0.8
norm_epsilon = 1e-05
masked_score = -1e+30

def head_group(queries, key_rows, values, lambdas, head_gain):
    length, head_count, doubled = queries.shape
    head_size = doubled // 2
    score_scale = head_size ** (-0.5)
    query_maps = queries.reshape(length, head_count, 2, head_size).astype(jnp.float32)
    key_maps = key_rows.reshape(length, head_count, 2, head_size).astype(jnp.float32)
    value_rows = values.astype(jnp.float32)
    block_size = math.gcd(length, 256)
    key_index = jnp.arange(length, dtype=jnp.int32)

    def one_block(block_index):
        offset = block_index * block_size
        query_block = lax.dynamic_slice_in_dim(query_maps, offset, block_size, 0)
        scores = jnp.einsum('qhmd,khmd->hmqk', query_block, key_maps) * score_scale
        query_index = offset + jnp.arange(block_size, dtype=jnp.int32)
        visible = key_index[None, :] <= query_index[:, None]
        scores = jnp.where(visible, scores, masked_score)
        highest = lax.optimization_barrier(jnp.max(scores, axis=-1, keepdims=True))
        weights = jnp.where(visible, jnp.exp(scores - highest), 0.0)
        totals = lax.optimization_barrier(jnp.sum(weights, axis=-1))
        rounded = lax.optimization_barrier(weights.astype(jnp.bfloat16)).astype(jnp.float32)
        map_out = jnp.einsum('hmqk,khe->hmqe', rounded, value_rows) / totals[..., None]
        combined = map_out[:, 0] - lambdas[:, None, None] * map_out[:, 1]
        mean_square = lax.optimization_barrier(jnp.mean(combined * combined, axis=-1, keepdims=True))
        normed = combined * lax.rsqrt(mean_square + norm_epsilon) * head_gain * branch_scale
        return jnp.transpose(normed, (1, 0, 2)).astype(jnp.bfloat16)
    blocks = lax.map(one_block, jnp.arange(length // block_size, dtype=jnp.int32))
    return blocks.reshape(length, head_count * values.shape[2])

def layer_norm(values, gains):
    centered = values - lax.optimization_barrier(jnp.mean(values, axis=-1, keepdims=True))
    variance = lax.optimization_barrier(jnp.mean(centered * centered, axis=-1, keepdims=True))
    return centered * lax.rsqrt(variance + norm_epsilon) * gains

def reference(residual, query_small, key_small, value_small, query_large, key_large, value_large, lambda_small, lambda_large, head_gain, output_small, output_large, norm_gain, gate_weight, up_weight, down_weight):
    attended_small = head_group(query_small, key_small, value_small, lambda_small, head_gain)
    attended_large = head_group(query_large, key_large, value_large, lambda_large, head_gain)
    mixed_sum = jnp.dot(attended_small, output_small, preferred_element_type=jnp.float32) + jnp.dot(attended_large, output_large, preferred_element_type=jnp.float32)
    pre_norm = residual_scale * residual.astype(jnp.float32) + mixed_sum
    normed = layer_norm(pre_norm, norm_gain).astype(jnp.bfloat16)
    gate_rows = jnp.dot(normed, gate_weight, preferred_element_type=jnp.float32)
    up_rows = jnp.dot(normed, up_weight, preferred_element_type=jnp.float32)
    hidden = (jax.nn.silu(gate_rows) * up_rows).astype(jnp.bfloat16)
    down_sum = jnp.dot(hidden, down_weight, preferred_element_type=jnp.float32)
    return (residual_scale * normed.astype(jnp.float32) + 0.5 * down_sum).astype(jnp.bfloat16)
```

```python
import functools

import jax
import jax.numpy as jnp
from jax import lax
from jax.experimental import pallas as pl
from jax.experimental.pallas import tpu as pltpu
from jax.sharding import PartitionSpec as P

residual_scale = 8.0**0.25
branch_scale = 0.8
norm_epsilon = 1e-05
masked_score = -1e30
log2_e = 1.4426950408889634
MESH = pl.DeviceIdType.MESH


def layer_norm(values, gains):
    centered = values - jnp.mean(values, axis=-1, keepdims=True)
    variance = jnp.mean(centered * centered, axis=-1, keepdims=True)
    return centered * lax.rsqrt(variance + norm_epsilon) * gains


def fold_lanes(values, op):
    result = values[:, :128]
    for start in range(128, values.shape[1], 128):
        result = op(result, values[:, start : start + 128])
    return result


class Plan:
    def __init__(self, n, m, small, large, tokens, rows, small_size, large_size):
        self.n, self.m = n, m
        self.slots = small + large
        self.group = n // self.slots
        half = small // 2
        self.kinds = [("s", i) for i in range(half)]
        self.kinds += [("l", i) for i in range(large)]
        self.kinds += [("s", i) for i in range(half, small)]
        self.keys = [1 if kind == "s" else 2 for kind, _ in self.kinds]
        self.starts = []
        at = 0
        for k in self.keys:
            self.starts.append(at)
            at += 2 * k + 1
        self.tokens, self.rows = tokens, rows
        self.small_size, self.large_size = small_size, large_size
        order = []
        lo, hi = 0, self.slots - 1
        while lo <= hi:
            order.append(hi)
            if lo < hi:
                order.append(lo)
            lo, hi = lo + 1, hi - 1
        self.order = order


def attend_kernel(plan, lam_ref, planes, gain_ref, att_ref, kv, q, o, att, peak, total, acc,
                  kvz_s, kvz_r, qz_s, qz_r, kvx_s, kvx_r, loc, o_s, o_r, o_l):
    slots, group, m = plan.slots, plan.group, plan.m
    tokens, rows = plan.tokens, plan.rows
    s = lax.axis_index("sp")
    t = lax.axis_index("tp")
    a, b = s // group, s % group
    aside = lax.rem(s + 1, plan.n)
    mine = pl.ds(pl.multiple_of(s * tokens, tokens), tokens)
    large = a < 0
    for i, k in enumerate(plan.keys):
        if k == 2:
            large = jnp.logical_or(large, a == i)
    by_kind = ((1, jnp.logical_not(large)), (2, large))

    def kv_z(i, to):
        k = plan.keys[i]
        return pltpu.make_async_remote_copy(
            src_ref=planes.at[pl.ds(plan.starts[i], k + 1)],
            dst_ref=kv.at[pl.ds(0, k + 1), mine],
            send_sem=kvz_s.at[i], recv_sem=kvz_r.at[a],
            device_id={"sp": to * group + b, "tp": t}, device_id_type=MESH)

    def q_z(i, to):
        k = plan.keys[i]
        return pltpu.make_async_remote_copy(
            src_ref=planes.at[pl.ds(plan.starts[i] + k + 1, k)],
            dst_ref=q.at[pl.ds(0, k), a],
            send_sem=qz_s.at[i], recv_sem=qz_r.at[a],
            device_id={"sp": to * group + b, "tp": t}, device_id_type=MESH)

    def kv_own(i):
        k = plan.keys[i]
        return pltpu.make_async_copy(
            planes.at[pl.ds(plan.starts[i], k + 1)], kv.at[pl.ds(0, k + 1), mine], loc.at[0])

    def q_own(i):
        k = plan.keys[i]
        return pltpu.make_async_copy(
            planes.at[pl.ds(plan.starts[i] + k + 1, k)], q.at[pl.ds(0, k), a], loc.at[1])

    def peer(j):
        return a * group + lax.rem(b + j, group)

    def kv_x(k, i, j):
        block = pl.ds(pl.multiple_of((i * group + b) * tokens, tokens), tokens)
        return pltpu.make_async_remote_copy(
            src_ref=kv.at[pl.ds(0, k + 1), block],
            dst_ref=kv.at[pl.ds(0, k + 1), block],
            send_sem=kvx_s.at[i, j - 1], recv_sem=kvx_r.at[i, j - 1],
            device_id={"sp": peer(j), "tp": t}, device_id_type=MESH)

    for i in range(slots):
        @pl.when(a == i)
        def _():
            kv_own(i).start()
            q_own(i).start()

    for i in plan.order:
        @pl.when(a != i)
        def _():
            kv_z(i, i).start()
    for i in plan.order:
        @pl.when(a != i)
        def _():
            q_z(i, i).start()

    for i in range(slots):
        @pl.when(a == i)
        def _():
            kv_own(i).wait()
            q_own(i).wait()

    for j in range(1, group):
        for i in range(slots):
            @pl.when(a == i)
            def _():
                kv_x(plan.keys[i], i, j).start()

    for distance in range(1, slots):
        for i in range(slots):
            @pl.when(jnp.abs(a - i) == distance)
            def _():
                for k, when in by_kind:
                    @pl.when(when)
                    def _():
                        source = pl.ds(pl.multiple_of((i * group + b) * tokens, tokens), tokens)
                        pltpu.make_async_remote_copy(
                            src_ref=kv.at[pl.ds(0, k + 1), source],
                            dst_ref=kv.at[pl.ds(0, k + 1), source],
                            send_sem=kvz_s.at[i], recv_sem=kvz_r.at[i],
                            device_id={"sp": aside, "tp": t}, device_id_type=MESH).wait_recv()
                        for j in range(1, group):
                            kv_x(k, i, j).start()

    for i in range(slots):
        for k, when in by_kind:
            @pl.when(when)
            def _():
                @pl.when(a != i)
                def _():
                    pltpu.make_async_remote_copy(
                        src_ref=q.at[pl.ds(0, k), i], dst_ref=q.at[pl.ds(0, k), i],
                        send_sem=qz_s.at[i], recv_sem=qz_r.at[i],
                        device_id={"sp": aside, "tp": t}, device_id_type=MESH).wait_recv()

                for j in range(1, group):
                    kv_x(k, i, j).wait_recv()

    @pl.when(jnp.logical_not(large))
    def _():
        for i in range(slots):
            both = q[0, i]
            lane = lax.broadcasted_iota(jnp.int32, both.shape, 1)
            q[1, i] = jnp.where(lane >= plan.small_size, both, jnp.zeros_like(both))
            q[0, i] = jnp.where(lane < plan.small_size, both, jnp.zeros_like(both))

    lift = large.astype(jnp.int32)
    factor = jnp.where(large, plan.large_size**-0.5 * log2_e, plan.small_size**-0.5 * log2_e)
    lam = lam_ref[a]
    last = (((1,), (1,)), ((), ()))
    high = min(256, tokens)
    parts = tokens // high
    owners = high // rows
    head = t * slots + a

    def o_copy(i, part, w):
        which = part * owners + w
        return pltpu.make_async_remote_copy(
            src_ref=o.at[i, pl.ds(pl.multiple_of(which * rows, rows), rows)],
            dst_ref=att.at[head],
            send_sem=o_s.at[i, which], recv_sem=o_r.at[head],
            device_id={"sp": i * group + b, "tp": which}, device_id_type=MESH)

    def attend(step, carry):
        i, part = step // parts, lax.rem(step, parts)
        block = i * group + b
        row0 = part * high
        here = pl.ds(pl.multiple_of(row0, high), high)
        queries = (q[0, i, here], q[1, i, here])

        def score(which, start):
            keys = kv[which * lift, pl.ds(pl.multiple_of(start, tokens), tokens)]
            return lax.dot_general(queries[which], keys, last, preferred_element_type=jnp.float32)

        def masked(which):
            near = score(which, block * tokens)
            row = row0 + lax.broadcasted_iota(jnp.int32, near.shape, 0)
            column = lax.broadcasted_iota(jnp.int32, near.shape, 1)
            return jnp.where(column <= row, near, masked_score)

        for which in range(2):
            peak[which] = fold_lanes(masked(which), jnp.maximum)

        def find(c, carry):
            for which in range(2):
                peak[which] = jnp.maximum(
                    peak[which], fold_lanes(score(which, c * tokens), jnp.maximum))
            return carry

        lax.fori_loop(0, block, find, 0)
        tops = [jnp.max(peak[which], axis=1, keepdims=True) for which in range(2)]
        for which in range(2):
            peak[which] = jnp.broadcast_to(tops[which], (high, 128))

        def weigh(which, values, start, first):
            top = peak[which][:, :1]
            weights = jnp.exp2((values - top) * factor)
            value = kv[1 + lift, pl.ds(pl.multiple_of(start, tokens), tokens)]
            part_sum = fold_lanes(weights, jnp.add)
            part_acc = jnp.dot(weights.astype(jnp.bfloat16), value, preferred_element_type=jnp.float32)
            if first:
                total[which] = part_sum
                acc[which] = part_acc
            else:
                total[which] += part_sum
                acc[which] += part_acc

        for which in range(2):
            weigh(which, masked(which), block * tokens, True)

        def far(c, carry):
            for which in range(2):
                weigh(which, score(which, c * tokens), c * tokens, False)
            return carry

        lax.fori_loop(0, block, far, 0)
        outs = [acc[which] / jnp.sum(total[which], axis=1, keepdims=True) for which in range(2)]
        combined = outs[0] - lam * outs[1]
        mean_square = jnp.mean(combined * combined, axis=1, keepdims=True)
        normed = combined * lax.rsqrt(mean_square + norm_epsilon) * gain_ref[...] * branch_scale
        o[i, here] = normed.astype(o.dtype)
        return carry

    def send(step, carry):
        i, part = step // parts, lax.rem(step, parts)
        for w in range(owners):
            self_here = jnp.logical_and(i == a, part * owners + w == t)

            @pl.when(jnp.logical_not(self_here))
            def _():
                o_copy(i, part, w).start()
        return carry

    steps = slots * parts

    def step_body(step, carry):
        attend(step, carry)

        @pl.when(step > 0)
        def _():
            send(step - 1, carry)

        return carry

    lax.fori_loop(0, steps, step_body, 0)
    att[head] = o[a, pl.ds(pl.multiple_of(t * rows, rows), rows)]
    send(steps - 1, 0)

    for h in range(m * slots):
        @pl.when(head != h)
        def _():
            pltpu.make_async_remote_copy(
                src_ref=att.at[h], dst_ref=att.at[h], send_sem=o_s.at[0, 0], recv_sem=o_r.at[h],
                device_id={"sp": aside, "tp": t}, device_id_type=MESH).wait_recv()
    att_ref[...] = att[...]

    for i in range(slots):
        @pl.when(a != i)
        def _():
            kv_z(i, i).wait_send()
            q_z(i, i).wait_send()

        for k, when in by_kind:
            @pl.when(when)
            def _():
                for j in range(1, group):
                    kv_x(k, i, j).wait_send()
        for part in range(parts):
            for w in range(owners):
                @pl.when(jnp.logical_not(jnp.logical_and(i == a, part * owners + w == t)))
                def _():
                    o_copy(i, part, w).wait_send()


def attend(plan, lams, planes, gain, width):
    dma = pltpu.SemaphoreType.DMA
    slots, n, m = plan.slots, plan.n, plan.m
    high = min(256, plan.tokens)
    any_space = pl.BlockSpec(memory_space=pl.ANY)
    vmem = pl.BlockSpec(memory_space=pltpu.VMEM)
    others = max(plan.group - 1, 1)
    return pl.pallas_call(
        functools.partial(attend_kernel, plan),
        out_shape=jax.ShapeDtypeStruct((m * slots, plan.rows, width), jnp.bfloat16),
        in_specs=[pl.BlockSpec(memory_space=pltpu.SMEM), any_space, vmem],
        out_specs=vmem,
        scratch_shapes=[
            pltpu.VMEM((3, n * plan.tokens, width), jnp.bfloat16),
            pltpu.VMEM((2, slots, plan.tokens, width), jnp.bfloat16),
            pltpu.VMEM((slots, plan.tokens, width), jnp.bfloat16),
            pltpu.VMEM((m * slots, plan.rows, width), jnp.bfloat16),
            pltpu.VMEM((2, high, 128), jnp.float32),
            pltpu.VMEM((2, high, 128), jnp.float32),
            pltpu.VMEM((2, high, width), jnp.float32),
            dma((slots,)), dma((slots,)), dma((slots,)), dma((slots,)),
            dma((slots, others)), dma((slots, others)),
            dma((2,)),
            dma((slots, plan.tokens // plan.rows)), dma((m * slots,)), dma,
        ],
        compiler_params=pltpu.CompilerParams(
            vmem_limit_bytes=60 * 2**20, has_side_effects=True),
        cost_estimate=pl.CostEstimate(
            flops=60_000_000_000, bytes_accessed=planes.size * 2, transcendentals=8_000_000),
        name="attend",
    )(lams, planes, gain.reshape(1, width))


def swap(value, axis, bit):
    pairs = [(i, i ^ (1 << bit)) for i in range(lax.axis_size(axis))]
    return lax.ppermute(value, axis, pairs)


def gather_rows(rows, bits):
    held = {0: rows}
    for bit in reversed(range(bits)):
        keys = sorted(held)
        sent = jnp.concatenate([held[k] for k in keys], axis=0) if len(keys) > 1 else held[0]
        got = swap(sent, "tp", bit)
        for i, k in enumerate(keys):
            held[k | (1 << bit)] = got[i * rows.shape[0] : (i + 1) * rows.shape[0]]
    return jnp.concatenate([held[k] for k in sorted(held)], axis=0)


def scatter_sum(values, bits):
    rows = values.shape[0] >> bits
    held = {k: values[k * rows : (k + 1) * rows] for k in range(1 << bits)}
    for bit in range(bits):
        kept = [k for k in sorted(held) if not k >> bit & 1]
        sent = [held[k | (1 << bit)].astype(jnp.bfloat16) for k in kept]
        got = swap(jnp.concatenate(sent, axis=0) if len(sent) > 1 else sent[0], "tp", bit)
        held = {
            k: held[k] + got[i * rows : (i + 1) * rows].astype(jnp.float32)
            for i, k in enumerate(kept)
        }
    return held[0]


def per_device(
    residual, query_small, key_small, value_small, query_large, key_large, value_large,
    lambda_small, lambda_large, head_gain, output_small, output_large, norm_gain,
    gate_weight, up_weight, down_weight,
):
    tokens, heads_small, width = value_small.shape
    heads_large = value_large.shape[1]
    rows, _ = residual.shape
    n, m = lax.axis_size("sp"), lax.axis_size("tp")
    bits = m.bit_length() - 1
    plan = Plan(n, m, heads_small, heads_large, tokens, rows,
                query_small.shape[2] // 2, query_large.shape[2] // 2)
    half = plan.large_size
    planes, lams, weights = [], [], []
    for kind, i in plan.kinds:
        if kind == "s":
            planes += [key_small[:, i], value_small[:, i], query_small[:, i]]
            lams.append(lambda_small[i])
            weights.append(output_small[i * width : (i + 1) * width])
        else:
            planes += [key_large[:, i, :half], key_large[:, i, half:], value_large[:, i],
                       query_large[:, i, :half], query_large[:, i, half:]]
            lams.append(lambda_large[i])
            weights.append(output_large[i * width : (i + 1) * width])
    output_full = lax.all_gather(jnp.concatenate(weights, axis=0), "tp", axis=0, tiled=True)
    gate_full = lax.all_gather(gate_weight, "sp", axis=0, tiled=True)
    up_full = lax.all_gather(up_weight, "sp", axis=0, tiled=True)
    down_full = lax.all_gather(down_weight, "sp", axis=1, tiled=True)
    attended = attend(plan, jnp.stack(lams), jnp.stack(planes), head_gain, width)
    attended = jnp.transpose(attended, (1, 0, 2)).reshape(rows, -1)
    mixed_sum = jnp.dot(attended, output_full, preferred_element_type=jnp.float32)
    normed = layer_norm(
        residual_scale * residual.astype(jnp.float32) + mixed_sum, norm_gain
    ).astype(jnp.bfloat16)
    whole_rows = gather_rows(normed, bits)
    gate_rows = jnp.dot(whole_rows, gate_full, preferred_element_type=jnp.float32)
    up_rows = jnp.dot(whole_rows, up_full, preferred_element_type=jnp.float32)
    hidden = (jax.nn.silu(gate_rows) * up_rows).astype(jnp.bfloat16)
    down_sum = scatter_sum(
        jnp.dot(hidden, down_full, preferred_element_type=jnp.float32), bits
    )
    return (residual_scale * normed.astype(jnp.float32) + 0.5 * down_sum).astype(jnp.bfloat16)


def solution(mesh):
    in_specs = (
        P(("sp", "tp"), None), P("sp", "tp", None), P("sp", "tp", None), P("sp", "tp", None),
        P("sp", "tp", None), P("sp", "tp", None), P("sp", "tp", None), P("tp"), P("tp"), P(),
        P("tp", None), P("tp", None), P(), P("sp", "tp"), P("sp", "tp"), P("tp", "sp"),
    )

    return jax.shard_map(
        per_device, mesh=mesh, in_specs=in_specs, out_specs=P(("sp", "tp"), None), check_vma=False
    )
```

```python
import functools

import jax
import jax.numpy as jnp
from jax import lax
from jax.experimental import pallas as pl
from jax.experimental.pallas import tpu as pltpu
from jax.sharding import PartitionSpec as P

residual_scale = 8.0**0.25
branch_scale = 0.8
norm_epsilon = 1e-05
masked_score = -1e30
log2_e = 1.4426950408889634
MESH = pl.DeviceIdType.MESH


def layer_norm(values, gains):
    centered = values - jnp.mean(values, axis=-1, keepdims=True)
    variance = jnp.mean(centered * centered, axis=-1, keepdims=True)
    return centered * lax.rsqrt(variance + norm_epsilon) * gains


def fold_lanes(values, op):
    result = values[:, :128]
    for start in range(128, values.shape[1], 128):
        result = op(result, values[:, start : start + 128])
    return result


class Plan:
    def __init__(self, n, m, small, large, tokens, rows, small_size, large_size):
        self.n, self.m = n, m
        self.slots = small + large
        self.group = n // self.slots
        half = small // 2
        self.kinds = [("s", i) for i in range(half)]
        self.kinds += [("l", i) for i in range(large)]
        self.kinds += [("s", i) for i in range(half, small)]
        self.keys = [1 if kind == "s" else 2 for kind, _ in self.kinds]
        self.starts = []
        at = 0
        for k in self.keys:
            self.starts.append(at)
            at += 2 * k + 1
        self.tokens, self.rows = tokens, rows
        self.small_size, self.large_size = small_size, large_size
        order = []
        lo, hi = 0, self.slots - 1
        while lo <= hi:
            order.append(hi)
            if lo < hi:
                order.append(lo)
            lo, hi = lo + 1, hi - 1
        self.order = order

    def mixer(self, features, units):
        tiles = units // 128
        first = (tiles + 1) // 2 * 128
        self.sizes, self.offsets = (first, units - first), (0, first)
        self.depth = features // self.n
        self.features = features
        self.chips = self.m // 2
        self.peers = 2 * self.chips


def layer_kernel(plan, lam_ref, planes, gain_ref, out_w, residual_ref, norm_ref, gate, up, down, out_ref,
                 kv, q, o, att, peak, total, acc, w_out, w_gate, w_up, w_down, x, hidden, mix,
                 send_half, got_half, kept, send_sum, got_sum,
                 kvz_s, kvz_r, qz_s, qz_r, kvx_s, kvx_r, loc, o_s, o_r,
                 wz_s, wz_r, wx_s, wx_r, own_w, wy_s, wy_r, wc_s, wc_r,
                 ag_s, ag_r, agc_s, agc_r, rc_s, rc_r, r2_s, r2_r):
    slots, group, m, n = plan.slots, plan.group, plan.m, plan.n
    tokens, rows, chips, depth = plan.tokens, plan.rows, plan.chips, plan.depth
    features = plan.features
    s = lax.axis_index("sp")
    t = lax.axis_index("tp")
    a, b = s // group, lax.rem(s, group)
    y, c = t // 2, lax.rem(t, 2)
    parity = lax.rem(a, 2)
    partner = y * 2 + 1 - c
    aside = lax.rem(s + 1, n)
    mine = pl.ds(pl.multiple_of(s * tokens, tokens), tokens)
    large = a < 0
    for i, k in enumerate(plan.keys):
        if k == 2:
            large = jnp.logical_or(large, a == i)
    by_kind = ((1, jnp.logical_not(large)), (2, large))
    by_parity = ((0, parity == 0), (1, parity == 1))

    def remote(src, dst, send, recv, sp, tp):
        return pltpu.make_async_remote_copy(
            src_ref=src, dst_ref=dst, send_sem=send, recv_sem=recv,
            device_id={"sp": sp, "tp": tp}, device_id_type=MESH)

    def arrival(dst, recv):
        remote(dst, dst, kvz_s.at[0], recv, aside, t).wait_recv()

    def block_of(i):
        return pl.ds(pl.multiple_of((i * group + b) * tokens, tokens), tokens)

    def kv_z(i):
        k = plan.keys[i]
        return remote(planes.at[pl.ds(plan.starts[i], k + 1)], kv.at[pl.ds(0, k + 1), mine],
                      kvz_s.at[i], kvz_r.at[a], i * group + b, t)

    def q_z(i):
        k = plan.keys[i]
        return remote(planes.at[pl.ds(plan.starts[i] + k + 1, k)], q.at[pl.ds(0, k), a],
                      qz_s.at[i], qz_r.at[a], i * group + b, t)

    def kv_own(i):
        k = plan.keys[i]
        return pltpu.make_async_copy(
            planes.at[pl.ds(plan.starts[i], k + 1)], kv.at[pl.ds(0, k + 1), mine], loc.at[0])

    def q_own(i):
        k = plan.keys[i]
        return pltpu.make_async_copy(
            planes.at[pl.ds(plan.starts[i] + k + 1, k)], q.at[pl.ds(0, k), a], loc.at[1])

    def peer(j):
        return a * group + lax.rem(b + j, group)

    def kv_x(k, i, j):
        part = kv.at[pl.ds(0, k + 1), block_of(i)]
        return remote(part, part, kvx_s.at[i, j - 1], kvx_r.at[i, j - 1], peer(j), t)

    pieces = 6

    def piece_in(k, par):
        tensor, h = k // 2, k % 2
        if tensor < 2:
            return (gate, up)[tensor].at[
                pl.ds(h * (depth // 2), depth // 2), pl.ds(plan.offsets[par], plan.sizes[par])]
        size = plan.sizes[par] // 2
        return down.at[pl.ds(plan.offsets[par] + h * size, size), :]

    def piece_at(k, par, block):
        tensor, h = k // 2, k % 2
        if tensor < 2:
            start = pl.multiple_of(block * depth + h * (depth // 2), depth // 2)
            return (w_gate, w_up)[tensor].at[pl.ds(start, depth // 2), pl.ds(0, plan.sizes[par])]
        size = plan.sizes[par] // 2
        return w_down.at[pl.ds(h * size, size), pl.ds(pl.multiple_of(block * depth, depth), depth)]

    def w_z(k, i):
        return remote(piece_in(k, i % 2), piece_at(k, i % 2, s), wz_s.at[k, i], wz_r.at[k, a],
                      i * group + b, t)

    def w_own(k, par):
        return pltpu.make_async_copy(piece_in(k, par), piece_at(k, par, s), own_w.at[k])

    def w_x(k, par, i, j):
        part = piece_at(k, par, i * group + b)
        return remote(part, part, wx_s.at[k, i, j - 1], wx_r.at[k, i, j - 1], peer(j), t)

    def w_start(k):
        for i in plan.order:
            @pl.when(a != i)
            def _():
                w_z(k, i).start()

    def w_forward(k):
        for par, when in by_parity:
            @pl.when(when)
            def _():
                for i in range(slots):
                    @pl.when(a == i)
                    def _():
                        w_own(k, par).wait()

                    @pl.when(a != i)
                    def _():
                        arrival(piece_at(k, par, i * group + b), wz_r.at[k, i])

                    for j in range(1, group):
                        w_x(k, par, i, j).start()

    def w_wait(k):
        for par, when in by_parity:
            @pl.when(when)
            def _():
                for i in range(slots):
                    for j in range(1, group):
                        block = i * group + lax.rem(b + group - j, group)
                        arrival(piece_at(k, par, block), wx_r.at[k, i, j - 1])

    def tp_of(dy):
        return lax.rem(y + dy, chips) * 2 + c

    def wo_y(dy):
        return remote(out_w, w_out.at[t], wy_s.at[dy - 1], wy_r.at[chips - dy - 1], s, tp_of(dy))

    def wo_c(dy):
        part = w_out.at[tp_of(dy)]
        return remote(out_w if dy == 0 else part, part, wc_s.at[dy], wc_r.at[dy], s, partner)

    def wo_own():
        return pltpu.make_async_copy(out_w, w_out.at[t], loc.at[2])

    def other(r):
        dz, dy = r // chips, r % chips
        slot = a + dz * (1 - 2 * parity)
        return slot * group + b, tp_of(dy)

    def back(r):
        dz, dy = r // chips, r % chips
        return dz * chips + (chips - dy) % chips

    def row_far(r):
        sp, tp = other(r)
        return remote(x.at[0, 0], x.at[back(r), 0], ag_s.at[r], ag_r.at[back(r)], sp, tp)

    def row_near(r):
        return remote(x.at[r, 0], x.at[r, 1], agc_s.at[r], agc_r.at[r], s, partner)

    def half_near(r):
        return remote(send_half.at[r], got_half.at[r], rc_s.at[r], rc_r.at[r], s, partner)

    def sum_far(r):
        sp, tp = other(r)
        return remote(send_sum.at[r], got_sum.at[back(r)], r2_s.at[r], r2_r.at[back(r)], sp, tp)

    for i in range(slots):
        @pl.when(a == i)
        def _():
            kv_own(i).start()
            q_own(i).start()
    for i in plan.order:
        @pl.when(a != i)
        def _():
            kv_z(i).start()
    for i in plan.order:
        @pl.when(a != i)
        def _():
            q_z(i).start()
    for dy in range(1, chips):
        wo_y(dy).start()
    wo_c(0).start()
    wo_own().start()
    for par, when in by_parity:
        @pl.when(when)
        def _():
            for k in range(pieces):
                w_own(k, par).start()
    if plan.sizes[1] < plan.sizes[0]:
        @pl.when(parity == 1)
        def _():
            spare = pl.ds(plan.sizes[1], plan.sizes[0] - plan.sizes[1])
            w_gate[:, spare] = jnp.zeros((features, plan.sizes[0] - plan.sizes[1]), w_gate.dtype)
            w_up[:, spare] = jnp.zeros((features, plan.sizes[0] - plan.sizes[1]), w_up.dtype)
            w_down[spare, :] = jnp.zeros((plan.sizes[0] - plan.sizes[1], features), w_down.dtype)

    for i in range(slots):
        @pl.when(a == i)
        def _():
            kv_own(i).wait()
            q_own(i).wait()
            for j in range(1, group):
                kv_x(plan.keys[i], i, j).start()

    w_start(0)

    for distance in range(1, slots):
        for i in range(slots):
            @pl.when(jnp.abs(a - i) == distance)
            def _():
                for k, when in by_kind:
                    @pl.when(when)
                    def _():
                        arrival(kv.at[pl.ds(0, k + 1), block_of(i)], kvz_r.at[i])
                        for j in range(1, group):
                            kv_x(k, i, j).start()
    w_start(1)

    for k, when in by_kind:
        @pl.when(when)
        def _():
            for i in range(slots):
                @pl.when(a != i)
                def _():
                    arrival(q.at[pl.ds(0, k), i], qz_r.at[i])

                for j in range(1, group):
                    block = i * group + lax.rem(b + group - j, group)
                    from_peer = pl.ds(pl.multiple_of(block * tokens, tokens), tokens)
                    arrival(kv.at[pl.ds(0, k + 1), from_peer], kvx_r.at[i, j - 1])

    @pl.when(jnp.logical_not(large))
    def _():
        for i in range(slots):
            both = q[0, i]
            lane = lax.broadcasted_iota(jnp.int32, both.shape, 1)
            q[1, i] = jnp.where(lane >= plan.small_size, both, jnp.zeros_like(both))
            q[0, i] = jnp.where(lane < plan.small_size, both, jnp.zeros_like(both))

    lift = large.astype(jnp.int32)
    factor = jnp.where(large, plan.large_size**-0.5 * log2_e, plan.small_size**-0.5 * log2_e)
    lam = lam_ref[a]
    last = (((1,), (1,)), ((), ()))
    high = min(256, tokens)
    parts = tokens // high
    owners = high // rows
    head = t * slots + a

    def o_copy(i, which):
        return remote(o.at[i, pl.ds(pl.multiple_of(which * rows, rows), rows)], att.at[head],
                      o_s.at[i, which], o_r.at[head], i * group + b, which)

    def attend(step):
        i, part = step // parts, lax.rem(step, parts)
        block = i * group + b
        row0 = part * high
        here = pl.ds(pl.multiple_of(row0, high), high)
        queries = (q[0, i, here], q[1, i, here])

        def score(which, start):
            keys = kv[which * lift, pl.ds(pl.multiple_of(start, tokens), tokens)]
            return lax.dot_general(queries[which], keys, last, preferred_element_type=jnp.float32)

        def masked(which):
            near = score(which, block * tokens)
            row = row0 + lax.broadcasted_iota(jnp.int32, near.shape, 0)
            column = lax.broadcasted_iota(jnp.int32, near.shape, 1)
            return jnp.where(column <= row, near, masked_score)

        for which in range(2):
            peak[which] = fold_lanes(masked(which), jnp.maximum)

        def find(chunk, carry):
            for which in range(2):
                peak[which] = jnp.maximum(
                    peak[which], fold_lanes(score(which, chunk * tokens), jnp.maximum))
            return carry

        lax.fori_loop(0, block, find, 0)
        tops = [jnp.max(peak[which], axis=1, keepdims=True) for which in range(2)]
        for which in range(2):
            peak[which] = jnp.broadcast_to(tops[which], (high, 128))

        def weigh(which, values, start, first):
            top = peak[which][:, :1]
            weights = jnp.exp2((values - top) * factor)
            value = kv[1 + lift, pl.ds(pl.multiple_of(start, tokens), tokens)]
            part_sum = fold_lanes(weights, jnp.add)
            part_acc = jnp.dot(weights.astype(jnp.bfloat16), value, preferred_element_type=jnp.float32)
            if first:
                total[which] = part_sum
                acc[which] = part_acc
            else:
                total[which] += part_sum
                acc[which] += part_acc

        for which in range(2):
            weigh(which, masked(which), block * tokens, True)

        def far(chunk, carry):
            for which in range(2):
                weigh(which, score(which, chunk * tokens), chunk * tokens, False)
            return carry

        lax.fori_loop(0, block, far, 0)
        outs = [acc[which] / jnp.sum(total[which], axis=1, keepdims=True) for which in range(2)]
        combined = outs[0] - lam * outs[1]
        mean_square = jnp.mean(combined * combined, axis=1, keepdims=True)
        normed = combined * lax.rsqrt(mean_square + norm_epsilon) * gain_ref[...] * branch_scale
        o[i, here] = normed.astype(o.dtype)

    def send(step):
        i, part = step // parts, lax.rem(step, parts)
        for w in range(owners):
            which = part * owners + w

            @pl.when(jnp.logical_not(jnp.logical_and(i == a, which == t)))
            def _():
                o_copy(i, which).start()

    steps = slots * parts
    plan_at = {}
    plan_at.setdefault(steps // 2, []).append(functools.partial(w_start, 2))
    plan_at.setdefault(steps * 5 // 8, []).append(functools.partial(w_forward, 0))
    plan_at.setdefault(steps * 7 // 8, []).append(functools.partial(w_forward, 1))

    def wo_forward():
        for dy in range(1, chips):
            arrival(w_out.at[tp_of(dy)], wy_r.at[dy - 1])
            wo_c(dy).start()

    plan_at.setdefault(steps * 6 // 8, []).append(wo_forward)

    def step_body(step, carry):
        for at, actions in plan_at.items():
            @pl.when(step == at)
            def _():
                for action in actions:
                    action()
        attend(step)

        @pl.when(step > 0)
        def _():
            send(step - 1)

        return carry

    lax.fori_loop(0, steps, step_body, 0)
    att[head] = o[a, pl.ds(pl.multiple_of(t * rows, rows), rows)]
    send(steps - 1)
    w_start(3)
    w_forward(2)

    wo_own().wait()
    for dy in range(chips):
        block = lax.rem(y + dy, chips) * 2 + 1 - c
        arrival(w_out.at[block], wc_r.at[dy])
    for h in range(m * slots):
        @pl.when(head != h)
        def _():
            arrival(att.at[h], o_r.at[h])
    wide = 512
    for start in range(0, features, wide):
        cols = pl.ds(start, wide)
        sums = None
        for tt in range(m):
            left = jnp.concatenate([att[tt * slots + i] for i in range(slots)], axis=1)
            term = jnp.dot(left, w_out[tt, :, cols], preferred_element_type=jnp.float32)
            sums = term if sums is None else sums + term
        mix[:, cols] = residual_scale * residual_ref[:, cols].astype(jnp.float32) + sums
    x[0, 0] = layer_norm(mix[...], norm_ref[...]).astype(x.dtype)
    for r in reversed(range(1, plan.peers)):
        row_far(r).start()
    row_near(0).start()
    w_start(4)
    w_start(5)
    w_forward(3)

    for k in range(4):
        w_wait(k)
    units = plan.sizes[0]
    span = 256 if units % 256 == 0 else 128

    def gate_up(r):
        both = x[r].reshape(2 * rows, features)
        for start in range(0, units, span):
            cols = pl.ds(start, span)
            g = jnp.dot(both, w_gate[:, cols], preferred_element_type=jnp.float32)
            u = jnp.dot(both, w_up[:, cols], preferred_element_type=jnp.float32)
            hidden[r, :, cols] = (g / (1.0 + jnp.exp(-g)) * u).astype(hidden.dtype)

    def gate_up_step(r, carry):
        @pl.when(r > 0)
        def _():
            arrival(x.at[r, 0], ag_r.at[r])
            row_near(r).start()

        arrival(x.at[r, 1], agc_r.at[r])
        gate_up(r)
        return carry

    lax.fori_loop(0, plan.peers, gate_up_step, 0)

    for k in (4, 5):
        w_forward(k)
    for k in (4, 5):
        w_wait(k)

    def down_rows(r):
        for start in range(0, features, wide):
            cols = pl.ds(start, wide)
            part = jnp.dot(hidden[r], w_down[:, cols], preferred_element_type=jnp.float32)
            kept[r, :, cols] = part[:rows]
            send_half[r, :, cols] = part[rows:].astype(send_half.dtype)

    def pass_on(r):
        arrival(got_half.at[r], rc_r.at[r])
        send_sum[r] = (kept[r] + got_half[r].astype(jnp.float32)).astype(send_sum.dtype)

    peers = plan.peers

    for back_r in range(peers):
        r = peers - 1 - back_r
        down_rows(r)
        half_near(r).start()
        if back_r > 0:
            pass_on(r + 1)
            sum_far(r + 1).start()
    arrival(got_half.at[0], rc_r.at[0])
    result = kept[0] + got_half[0].astype(jnp.float32)
    for r in range(1, peers):
        arrival(got_sum.at[r], r2_r.at[r])
        result += got_sum[r].astype(jnp.float32)
    out_ref[...] = (
        residual_scale * x[0, 0].astype(jnp.float32) + 0.5 * result).astype(out_ref.dtype)

    for i in range(slots):
        @pl.when(a != i)
        def _():
            kv_z(i).wait_send()
            q_z(i).wait_send()
            for k in range(pieces):
                w_z(k, i).wait_send()

        for k, when in by_kind:
            @pl.when(when)
            def _():
                for j in range(1, group):
                    kv_x(k, i, j).wait_send()
        for par, when in by_parity:
            @pl.when(when)
            def _():
                for j in range(1, group):
                    for k in range(pieces):
                        w_x(k, par, i, j).wait_send()
        for which in range(parts * owners):
            @pl.when(jnp.logical_not(jnp.logical_and(i == a, which == t)))
            def _():
                o_copy(i, which).wait_send()
    for dy in range(1, chips):
        wo_y(dy).wait_send()
    for dy in range(chips):
        wo_c(dy).wait_send()
    for r in range(peers):
        row_near(r).wait_send()
        half_near(r).wait_send()
        if r > 0:
            row_far(r).wait_send()
            sum_far(r).wait_send()


def run_layer(plan, lams, planes, gain, out_w, residual, norm_gain, gate, up, down, width):
    dma = pltpu.SemaphoreType.DMA
    slots, n, m, peers, chips = plan.slots, plan.n, plan.m, plan.peers, plan.chips
    rows, features, units = plan.rows, plan.features, plan.sizes[0]
    high = min(256, plan.tokens)
    anywhere = pl.BlockSpec(memory_space=pl.ANY)
    vmem = pl.BlockSpec(memory_space=pltpu.VMEM)
    others = max(plan.group - 1, 1)
    bf16, f32 = jnp.bfloat16, jnp.float32
    return pl.pallas_call(
        functools.partial(layer_kernel, plan),
        out_shape=jax.ShapeDtypeStruct((rows, features), bf16),
        in_specs=[pl.BlockSpec(memory_space=pltpu.SMEM), anywhere, vmem, anywhere, vmem, vmem,
                  anywhere, anywhere, anywhere],
        out_specs=vmem,
        scratch_shapes=[
            pltpu.VMEM((3, n * plan.tokens, width), bf16),
            pltpu.VMEM((2, slots, plan.tokens, width), bf16),
            pltpu.VMEM((slots, plan.tokens, width), bf16),
            pltpu.VMEM((m * slots, rows, width), bf16),
            pltpu.VMEM((2, high, 128), f32),
            pltpu.VMEM((2, high, 128), f32),
            pltpu.VMEM((2, high, width), f32),
            pltpu.VMEM((m, slots * width, features), bf16),
            pltpu.VMEM((features, units), bf16),
            pltpu.VMEM((features, units), bf16),
            pltpu.VMEM((units, features), bf16),
            pltpu.VMEM((peers, 2, rows, features), bf16),
            pltpu.VMEM((peers, 2 * rows, units), bf16),
            pltpu.VMEM((rows, features), f32),
            pltpu.VMEM((peers, rows, features), bf16),
            pltpu.VMEM((peers, rows, features), bf16),
            pltpu.VMEM((peers, rows, features), f32),
            pltpu.VMEM((peers, rows, features), bf16),
            pltpu.VMEM((peers, rows, features), bf16),
            dma((slots,)), dma((slots,)), dma((slots,)), dma((slots,)),
            dma((slots, others)), dma((slots, others)),
            dma((3,)),
            dma((slots, plan.tokens // rows)), dma((m * slots,)),
            dma((6, slots)), dma((6, slots)), dma((6, slots, others)), dma((6, slots, others)),
            dma((6,)),
            dma((max(chips - 1, 1),)), dma((max(chips - 1, 1),)), dma((chips,)), dma((chips,)),
            dma((peers,)), dma((peers,)), dma((peers,)), dma((peers,)),
            dma((peers,)), dma((peers,)), dma((peers,)), dma((peers,)),
        ],
        compiler_params=pltpu.CompilerParams(
            vmem_limit_bytes=60 * 2**20, has_side_effects=True),
        cost_estimate=pl.CostEstimate(
            flops=60_000_000_000, bytes_accessed=planes.size * 2, transcendentals=8_000_000),
        name="layer",
    )(lams, planes, gain.reshape(1, width), out_w, residual, norm_gain.reshape(1, features),
      gate, up, down)


def per_device(
    residual, query_small, key_small, value_small, query_large, key_large, value_large,
    lambda_small, lambda_large, head_gain, output_small, output_large, norm_gain,
    gate_weight, up_weight, down_weight,
):
    tokens, heads_small, width = value_small.shape
    heads_large = value_large.shape[1]
    rows, features = residual.shape
    n, m = lax.axis_size("sp"), lax.axis_size("tp")
    plan = Plan(n, m, heads_small, heads_large, tokens, rows,
                query_small.shape[2] // 2, query_large.shape[2] // 2)
    half = plan.large_size
    planes, lams, weights = [], [], []
    for kind, i in plan.kinds:
        if kind == "s":
            planes += [key_small[:, i], value_small[:, i], query_small[:, i]]
            lams.append(lambda_small[i])
            weights.append(output_small[i * width : (i + 1) * width])
        else:
            planes += [key_large[:, i, :half], key_large[:, i, half:], value_large[:, i],
                       query_large[:, i, :half], query_large[:, i, half:]]
            lams.append(lambda_large[i])
            weights.append(output_large[i * width : (i + 1) * width])
    short = -gate_weight.shape[1] % 128
    if short:
        gate_weight = jnp.pad(gate_weight, ((0, 0), (0, short)))
        up_weight = jnp.pad(up_weight, ((0, 0), (0, short)))
        down_weight = jnp.pad(down_weight, ((0, short), (0, 0)))
    plan.mixer(features, gate_weight.shape[1])
    return run_layer(
        plan, jnp.stack(lams), jnp.stack(planes), head_gain, jnp.concatenate(weights, axis=0),
        residual, norm_gain, gate_weight, up_weight, down_weight, width)


def solution(mesh):
    in_specs = (
        P(("sp", "tp"), None), P("sp", "tp", None), P("sp", "tp", None), P("sp", "tp", None),
        P("sp", "tp", None), P("sp", "tp", None), P("sp", "tp", None), P("tp"), P("tp"), P(),
        P("tp", None), P("tp", None), P(), P("sp", "tp"), P("sp", "tp"), P("tp", "sp"),
    )

    return jax.shard_map(
        per_device, mesh=mesh, in_specs=in_specs, out_specs=P(("sp", "tp"), None), check_vma=False
    )
```

```python
import functools

import jax
import jax.numpy as jnp
from jax import lax
from jax.experimental import pallas as pl
from jax.experimental.pallas import tpu as pltpu
from jax.sharding import PartitionSpec as P

residual_scale = 8.0**0.25
branch_scale = 0.8
norm_epsilon = 1e-05
masked_score = -1e30
log2_e = 1.4426950408889634
MESH = pl.DeviceIdType.MESH


def layer_norm(values, gains):
    centered = values - jnp.mean(values, axis=-1, keepdims=True)
    variance = jnp.mean(centered * centered, axis=-1, keepdims=True)
    return centered * lax.rsqrt(variance + norm_epsilon) * gains


def fold_lanes(values, op):
    result = values[:, :128]
    for start in range(128, values.shape[1], 128):
        result = op(result, values[:, start : start + 128])
    return result


class Plan:
    def __init__(self, n, m, small, large, tokens, rows, small_size, large_size, features, units):
        self.n, self.m, self.chips, self.peers = n, m, m // 2, m
        self.slots = small + large
        self.group = n // self.slots
        half = small // 2
        self.kinds = [("s", i) for i in range(half)]
        self.kinds += [("l", i) for i in range(large)]
        self.kinds += [("s", i) for i in range(half, small)]
        self.keys = [1 if kind == "s" else 2 for kind, _ in self.kinds]
        self.natural = [self.kinds.index(("s", i)) for i in range(small)]
        self.natural += [self.kinds.index(("l", i)) for i in range(large)]
        self.tokens, self.rows, self.features = tokens, rows, features
        self.small_size, self.large_size = small_size, large_size
        tiles = units // 128
        first = (tiles + 1) // 2 * 128
        self.sizes, self.offsets = (first, units - first), (0, first)
        self.depth = features // n
        self.halves = max(1, self.depth // 128)
        self.span = self.depth // self.halves
        self.columns = [(start, tuple(max(0, min(256, size - start)) for size in self.sizes))
                        for start in range(0, first, 256)]
        self.pieces = [(tensor, j) for j in range(len(self.columns)) for tensor in (0, 1)]
        self.ups = len(self.pieces)
        self.pieces += [(2, (h, part)) for h in range(self.halves) for part in range(2)]
        keys = n * tokens
        self.high = tokens
        while self.high > 128 and self.high * keys > 2**21:
            self.high //= 2


def layer_kernel(plan, lam_small, lam_large, k_small, v_small, q_small, k_large, v_large, q_large, gain_ref,
                 out_small, out_large, residual_ref, norm_ref, gate, up, down, out_ref,
                 kv, q, o, att, pool, peak, total, acc, w_out, w_gate, w_up, w_down, x, hidden,
                 send_half, got_half, send_sum, got_sum,
                 kz_s, kz_r, vz_s, vz_r, qz_s, qz_r, kx_s, kx_r, vx_s, vx_r, loc, o_s, o_r,
                 wz_s, wz_r, wx_s, wx_r, own_w, wy_s, wy_r, wc_s, wc_r,
                 ag_s, ag_r, agc_s, agc_r, rc_s, rc_r, r2_s, r2_r):
    slots, group, m, n = plan.slots, plan.group, plan.m, plan.n
    tokens, rows, chips, depth = plan.tokens, plan.rows, plan.chips, plan.depth
    features = plan.features
    s = lax.axis_index("sp")
    t = lax.axis_index("tp")
    a, b = s // group, lax.rem(s, group)
    y, c = t // 2, lax.rem(t, 2)
    parity = lax.rem(a, 2)
    partner = y * 2 + 1 - c
    aside = lax.rem(s + 1, n)
    mine = pl.ds(pl.multiple_of(s * tokens, tokens), tokens)
    large = a < 0
    for i, k in enumerate(plan.keys):
        if k == 2:
            large = jnp.logical_or(large, a == i)
    by_kind = ((1, jnp.logical_not(large)), (2, large))
    by_parity = ((0, parity == 0), (1, parity == 1))

    def remote(src, dst, send, recv, sp, tp):
        return pltpu.make_async_remote_copy(
            src_ref=src, dst_ref=dst, send_sem=send, recv_sem=recv,
            device_id={"sp": sp, "tp": tp}, device_id_type=MESH)

    def arrival(dst, recv):
        remote(dst, dst, kz_s.at[0], recv, aside, t).wait_recv()

    def block_of(i):
        return pl.ds(pl.multiple_of((i * group + b) * tokens, tokens), tokens)

    def source(i, what):
        kind, index = plan.kinds[i]
        return {"s": (k_small, v_small, q_small), "l": (k_large, v_large, q_large)}[kind][what].at[index]

    def to_slot(i, what):
        keys = pl.ds(0, plan.keys[i])
        dst = (kv.at[keys, mine], kv.at[pl.ds(2, 1), mine], q.at[keys, a])[what]
        send, recv = ((kz_s, kz_r), (vz_s, vz_r), (qz_s, qz_r))[what]
        return remote(source(i, what), dst, send.at[i], recv.at[a], i * group + b, t)

    def to_self(i, what):
        keys = pl.ds(0, plan.keys[i])
        dst = (kv.at[keys, mine], kv.at[pl.ds(2, 1), mine], q.at[keys, a])[what]
        return pltpu.make_async_copy(source(i, what), dst, loc.at[what])

    def peer(j):
        return a * group + lax.rem(b + j, group)

    def k_x(k, i, j):
        part = kv.at[pl.ds(0, k), block_of(i)]
        return remote(part, part, kx_s.at[i, j - 1], kx_r.at[i, j - 1], peer(j), t)

    def v_x(i, j):
        part = kv.at[pl.ds(2, 1), block_of(i)]
        return remote(part, part, vx_s.at[i, j - 1], vx_r.at[i, j - 1], peer(j), t)

    pieces = len(plan.pieces)

    def piece_in(k, par):
        tensor, which = plan.pieces[k]
        if tensor < 2:
            start, widths = plan.columns[which]
            return (gate, up)[tensor].at[:, pl.ds(plan.offsets[par] + start, widths[par])]
        h, part = which
        size = plan.sizes[par] // 2
        return down.at[pl.ds(plan.offsets[par] + part * size, size), pl.ds(h * plan.span, plan.span)]

    def piece_at(k, par, block):
        tensor, which = plan.pieces[k]
        if tensor < 2:
            start, widths = plan.columns[which]
            return (w_gate, w_up)[tensor].at[
                pl.ds(pl.multiple_of(block * depth, depth), depth), pl.ds(start, widths[par])]
        h, part = which
        size = plan.sizes[par] // 2
        return w_down.at[h, pl.ds(part * size, size),
                         pl.ds(pl.multiple_of(block * plan.span, plan.span), plan.span)]

    def w_z(k, i):
        return remote(piece_in(k, i % 2), piece_at(k, i % 2, s), wz_s.at[k, i], wz_r.at[k, a],
                      i * group + b, t)

    def w_own(k, par):
        return pltpu.make_async_copy(piece_in(k, par), piece_at(k, par, s), own_w.at[k])

    def w_x(k, par, i, j):
        part = piece_at(k, par, i * group + b)
        return remote(part, part, wx_s.at[k, i, j - 1], wx_r.at[k, i, j - 1], peer(j), t)

    def w_start(k):
        for distance in range(1, slots):
            for i in range(slots):
                @pl.when(jnp.abs(a - i) == distance)
                def _():
                    w_z(k, i).start()

    def w_share(k):
        for par, when in by_parity:
            @pl.when(when)
            def _():
                w_own(k, par).wait()
                for i in range(slots):
                    @pl.when(a == i)
                    def _():
                        for j in range(1, group):
                            w_x(k, par, i, j).start()

    def w_forward(k):
        for par, when in by_parity:
            @pl.when(when)
            def _():
                for distance in range(1, slots):
                    for i in range(slots):
                        @pl.when(jnp.abs(a - i) == distance)
                        def _():
                            arrival(piece_at(k, par, i * group + b), wz_r.at[k, i])
                            for j in range(1, group):
                                w_x(k, par, i, j).start()

    def w_wait(k):
        for par, when in by_parity:
            @pl.when(when)
            def _():
                for i in range(slots):
                    for j in range(1, group):
                        block = i * group + lax.rem(b + group - j, group)
                        arrival(piece_at(k, par, block), wx_r.at[k, i, j - 1])

    def tp_of(dy):
        return lax.rem(y + dy, chips) * 2 + c

    cut = out_small.shape[0]
    spans = ((out_small, pl.ds(0, cut)), (out_large, pl.ds(cut, out_large.shape[0])))

    def wo_y(dy, e):
        part, place = spans[e]
        return remote(part, w_out.at[t, place], wy_s.at[dy - 1, e], wy_r.at[chips - dy - 1, e], s, tp_of(dy))

    def wo_c(dy, e):
        part, place = spans[e]
        there = w_out.at[tp_of(dy), place]
        return remote(part if dy == 0 else there, there, wc_s.at[dy, e], wc_r.at[dy, e], s, partner)

    def wo_own(e):
        part, place = spans[e]
        return pltpu.make_async_copy(part, w_out.at[t, place], loc.at[3 + e])

    pair = (a + 1 - 2 * parity) * group + b

    def row_z():
        return remote(x.at[0, 0], x.at[chips, 0], ag_s.at[0], ag_r.at[chips], pair, t)

    def row_y(dz, dy):
        r = dz * chips + dy
        into = dz * chips + chips - dy
        return remote(x.at[dz * chips, 0], x.at[into, 0], ag_s.at[r], ag_r.at[into], s, tp_of(dy))

    def row_near(r):
        return remote(x.at[r, 0], x.at[r, 1], agc_s.at[r], agc_r.at[r], s, partner)

    def half_near(h, r):
        return remote(send_half.at[h, r], got_half.at[h, r], rc_s.at[h, r], rc_r.at[h, r], s, partner)

    def sum_y(h, dz, dy):
        into = dz * chips + chips - dy
        r = dz * chips + dy
        return remote(send_sum.at[h, r], got_sum.at[h, into], r2_s.at[h, r], r2_r.at[h, into], s, tp_of(dy))

    def sum_z(h):
        return remote(send_sum.at[h, chips], got_sum.at[h, 0], r2_s.at[h, 0], r2_r.at[h, 0], pair, t)

    barrier = pltpu.get_barrier_semaphore()
    for i in range(slots):
        for tt in range(m):
            @pl.when(jnp.logical_not(jnp.logical_and(i == a, tt == t)))
            def _():
                pl.semaphore_signal(barrier, inc=1, device_id={"sp": i * group + b, "tp": tt},
                                    device_id_type=MESH)
    for j in range(1, group):
        pl.semaphore_signal(barrier, inc=1, device_id={"sp": peer(j), "tp": t}, device_id_type=MESH)
    for i in range(slots):
        @pl.when(a == i)
        def _():
            for what in range(3):
                to_self(i, what).start()
    for e in range(2):
        wo_own(e).start()
    for par, when in by_parity:
        @pl.when(when)
        def _():
            for k in range(pieces):
                w_own(k, par).start()
    pl.semaphore_wait(barrier, slots * m - 1 + group - 1)

    for what in range(3):
        for distance in range(1, slots):
            for i in range(slots):
                @pl.when(jnp.abs(a - i) == distance)
                def _():
                    to_slot(i, what).start()
    w_start(0)
    for e in range(2):
        for dy in range(1, chips):
            wo_y(dy, e).start()
        wo_c(0, e).start()
    if plan.sizes[1] < plan.sizes[0]:
        @pl.when(parity == 1)
        def _():
            spare = pl.ds(plan.sizes[1], plan.sizes[0] - plan.sizes[1])
            w_gate[:, spare] = jnp.zeros((features, plan.sizes[0] - plan.sizes[1]), w_gate.dtype)
            w_up[:, spare] = jnp.zeros((features, plan.sizes[0] - plan.sizes[1]), w_up.dtype)
            for h in range(plan.halves):
                w_down[h, spare, :] = jnp.zeros(
                    (plan.sizes[0] - plan.sizes[1], features // plan.halves), w_down.dtype)

    for i in range(slots):
        @pl.when(a == i)
        def _():
            for what in range(3):
                to_self(i, what).wait()
            for j in range(1, group):
                k_x(plan.keys[i], i, j).start()
                v_x(i, j).start()

    for distance in range(1, slots):
        for i in range(slots):
            for k, when in by_kind:
                @pl.when(jnp.logical_and(when, jnp.abs(a - i) == distance))
                def _():
                    arrival(kv.at[pl.ds(0, k), block_of(i)], kz_r.at[i])
                    for j in range(1, group):
                        k_x(k, i, j).start()
    for distance in range(1, slots):
        for i in range(slots):
            @pl.when(jnp.abs(a - i) == distance)
            def _():
                arrival(kv.at[pl.ds(2, 1), block_of(i)], vz_r.at[i])
                for j in range(1, group):
                    v_x(i, j).start()

    w_start(1)
    w_start(2)
    for k in range(pieces):
        w_share(k)

    def ready(i):
        for k, when in by_kind:
            @pl.when(when)
            def _():
                @pl.when(a != i)
                def _():
                    arrival(q.at[pl.ds(0, k), i], qz_r.at[i])

                for j in range(1, group):
                    block = i * group + lax.rem(b + group - j, group)
                    from_peer = pl.ds(pl.multiple_of(block * tokens, tokens), tokens)
                    arrival(kv.at[pl.ds(0, k), from_peer], kx_r.at[i, j - 1])
                    arrival(kv.at[pl.ds(2, 1), from_peer], vx_r.at[i, j - 1])

        @pl.when(jnp.logical_not(large))
        def _():
            both = q[0, i]
            lane = lax.broadcasted_iota(jnp.int32, both.shape, 1)
            q[1, i] = jnp.where(lane >= plan.small_size, both, jnp.zeros_like(both))
            q[0, i] = jnp.where(lane < plan.small_size, both, jnp.zeros_like(both))

    lift = large.astype(jnp.int32)
    factor = jnp.where(large, plan.large_size**-0.5 * log2_e, plan.small_size**-0.5 * log2_e)
    lam = jnp.float32(0.0)
    for i, (kind, index) in enumerate(plan.kinds):
        lam = jnp.where(a == i, (lam_small if kind == "s" else lam_large)[index], lam)
    last = (((1,), (1,)), ((), ()))
    high = plan.high
    parts = tokens // high
    wide = group * tokens
    strip = min(512, tokens)
    head = t * slots + a

    def o_copy(i, which):
        return remote(o.at[i, pl.ds(pl.multiple_of(which * rows, rows), rows)], att.at[head],
                      o_s.at[i, which], o_r.at[head], i * group + b, which)

    def attend(i, part):
        row0 = part * high
        here = pl.ds(pl.multiple_of(row0, high), high)
        queries = (q[0, i, here], q[1, i, here])

        def find(chunk, last_one):
            for which in range(2):
                for off in range(0, wide, strip):
                    at = pl.ds(pl.multiple_of(chunk * wide + off, strip), strip)
                    score = lax.dot_general(
                        queries[which], kv[which * lift, at], last, preferred_element_type=jnp.float32)
                    if last_one:
                        row = b * tokens + row0 + lax.broadcasted_iota(jnp.int32, score.shape, 0)
                        column = off + lax.broadcasted_iota(jnp.int32, score.shape, 1)
                        score = jnp.where(column <= row, score, masked_score)
                    pool[which, :, at] = score
                    top = fold_lanes(score, jnp.maximum)
                    fresh = last_one and off == 0
                    peak[which] = top if fresh else jnp.maximum(peak[which], top)

        find(i, True)
        lax.fori_loop(0, i, lambda chunk, carry: find(chunk, False) or carry, 0)
        for which in range(2):
            peak[which] = jnp.broadcast_to(
                jnp.max(peak[which], axis=1, keepdims=True), (high, 128))

        def weigh(chunk, fresh):
            for which in range(2):
                sums = outs = None
                for off in range(0, wide, strip):
                    at = pl.ds(pl.multiple_of(chunk * wide + off, strip), strip)
                    score = pool[which, :, at]
                    top = peak[which]
                    weights = jnp.concatenate(
                        [jnp.exp2((score[:, u : u + 128] - top) * factor) for u in range(0, strip, 128)],
                        axis=1)
                    part_sum = fold_lanes(weights, jnp.add)
                    part_out = jnp.dot(
                        weights.astype(jnp.bfloat16), kv[2, at], preferred_element_type=jnp.float32)
                    sums = part_sum if sums is None else sums + part_sum
                    outs = part_out if outs is None else outs + part_out
                if fresh:
                    total[which], acc[which] = sums, outs
                else:
                    total[which] += sums
                    acc[which] += outs

        weigh(i, True)
        lax.fori_loop(0, i, lambda chunk, carry: weigh(chunk, False) or carry, 0)
        outs = [acc[which] / jnp.sum(total[which], axis=1, keepdims=True) for which in range(2)]
        combined = outs[0] - lam * outs[1]
        mean_square = jnp.mean(combined * combined, axis=1, keepdims=True)
        normed = combined * lax.rsqrt(mean_square + norm_epsilon) * gain_ref[...] * branch_scale
        o[i, here] = normed.astype(o.dtype)

    def send(i):
        for which in range(tokens // rows):
            @pl.when(jnp.logical_not(jnp.logical_and(i == a, which == t)))
            def _():
                o_copy(i, which).start()

    def wo_forward():
        for dy in range(1, chips):
            for e in range(2):
                place = spans[e][1]
                arrival(w_out.at[tp_of(dy), place], wy_r.at[dy - 1, e])
                wo_c(dy, e).start()

    def step_body(i, carry):
        for at in range(slots):
            @pl.when(i == at)
            def _():
                ready(at)
        lax.fori_loop(0, parts, lambda part, c: attend(i, part) or c, 0)

        @pl.when(i > 0)
        def _():
            send(i - 1)

        return carry

    lax.fori_loop(0, slots, step_body, 0)
    att[head] = o[a, pl.ds(pl.multiple_of(t * rows, rows), rows)]
    send(slots - 1)
    w_start(3)
    w_start(4)
    w_forward(0)
    wo_forward()
    w_forward(1)

    for e in range(2):
        wo_own(e).wait()
        for dy in range(chips):
            block = lax.rem(y + dy, chips) * 2 + 1 - c
            arrival(w_out.at[block, spans[e][1]], wc_r.at[dy, e])
    for h in range(m * slots):
        @pl.when(head != h)
        def _():
            arrival(att.at[h], o_r.at[h])
    stretch = 512
    base = plan.features
    for start in range(0, features, stretch):
        cols = pl.ds(start, stretch)
        sums = None
        for tt in range(m):
            left = jnp.concatenate([att[tt * slots + i] for i in plan.natural], axis=1)
            term = jnp.dot(left, w_out[tt, :, cols], preferred_element_type=jnp.float32)
            sums = term if sums is None else sums + term
        pool[1, pl.ds(0, rows), pl.ds(base + start, stretch)] = (
            residual_scale * residual_ref[:, cols].astype(jnp.float32) + sums)
    x[0, 0] = layer_norm(pool[1, pl.ds(0, rows), pl.ds(base, features)], norm_ref[...]).astype(x.dtype)
    peers = plan.peers
    row_z().start()
    for dy in range(1, chips):
        row_y(0, dy).start()
    row_near(0).start()
    for k in range(5, pieces):
        w_start(k)
    for k in range(2, plan.ups):
        w_forward(k)
    arrival(x.at[chips, 0], ag_r.at[chips])
    for dy in range(1, chips):
        row_y(1, dy).start()
    row_near(chips).start()
    w_forward(plan.ups)
    for dz in range(2):
        for dy in range(1, chips):
            r = dz * chips + dy
            arrival(x.at[r, 0], ag_r.at[r])
            row_near(r).start()
    w_forward(plan.ups + 1)
    for r in range(peers):
        arrival(x.at[r, 1], agc_r.at[r])

    def gate_up(j):
        start, widths = plan.columns[j]
        cols = pl.ds(start, max(widths))

        def one(r, carry):
            both = x[r].reshape(2 * rows, features)
            g = jnp.dot(both, w_gate[:, cols], preferred_element_type=jnp.float32)
            u = jnp.dot(both, w_up[:, cols], preferred_element_type=jnp.float32)
            hidden[r, :, cols] = (g / (1.0 + jnp.exp(-g)) * u).astype(hidden.dtype)
            return carry

        lax.fori_loop(0, peers, one, 0)

    done = plan.ups + 2
    for j in range(len(plan.columns)):
        w_wait(2 * j)
        w_wait(2 * j + 1)
        gate_up(j)
        if done < pieces and j + 1 < len(plan.columns):
            w_forward(done)
            done += 1

    low = features // plan.halves
    band = min(512, low)
    per_plane = high // rows

    def kept(r, cols):
        return pool.at[r // per_plane, pl.ds(r % per_plane * rows, rows), cols]

    def down_rows(h, r):
        for start in range(0, low, band):
            cols = pl.ds(start, band)
            part = jnp.dot(hidden[r], w_down[h, :, cols], preferred_element_type=jnp.float32)
            kept(r, pl.ds(h * low + start, band))[...] = part[:rows]
            send_half[h, r, :, cols] = part[rows:].astype(send_half.dtype)

    def near_sum(h, r):
        arrival(got_half.at[h, r], rc_r.at[h, r])
        return kept(r, pl.ds(h * low, low))[...] + got_half[h, r].astype(jnp.float32)

    def down_half(h):
        order = [dz * chips + dy for dz in (1, 0) for dy in list(range(1, chips)) + [0]]
        for r in order:
            down_rows(h, r)
            half_near(h, r).start()
        for r in order:
            if r % chips:
                send_sum[h, r] = near_sum(h, r).astype(send_sum.dtype)
                sum_y(h, r // chips, r % chips).start()

    def plane_sum(h, dz):
        result = near_sum(h, dz * chips)
        for dy in range(1, chips):
            r = dz * chips + dy
            arrival(got_sum.at[h, r], r2_r.at[h, r])
            result += got_sum[h, r].astype(jnp.float32)
        return result

    def pass_pair(h):
        send_sum[h, chips] = plane_sum(h, 1).astype(send_sum.dtype)
        sum_z(h).start()

    def finish(h):
        result = plane_sum(h, 0)
        arrival(got_sum.at[h, 0], r2_r.at[h, 0])
        result += got_sum[h, 0].astype(jnp.float32)
        for block in range(n):
            cols = pl.ds(block * depth + h * plan.span, plan.span)
            out_ref[:, cols] = (
                residual_scale * x[0, 0, :, cols].astype(jnp.float32)
                + 0.5 * result[:, block * plan.span : (block + 1) * plan.span]
            ).astype(out_ref.dtype)

    for h in range(plan.halves):
        first = plan.ups + 2 * h
        for k in range(done, first + 2):
            w_forward(k)
        done = max(done, first + 2)
        w_wait(first)
        w_wait(first + 1)
        if h > 0:
            pass_pair(h - 1)
        down_half(h)
    pass_pair(plan.halves - 1)
    for h in range(plan.halves):
        finish(h)

    for i in range(slots):
        @pl.when(a != i)
        def _():
            for what in range(3):
                to_slot(i, what).wait_send()
            for k in range(pieces):
                w_z(k, i).wait_send()

        for k, when in by_kind:
            @pl.when(when)
            def _():
                for j in range(1, group):
                    k_x(k, i, j).wait_send()
                    v_x(i, j).wait_send()
        for par, when in by_parity:
            @pl.when(when)
            def _():
                for j in range(1, group):
                    for k in range(pieces):
                        w_x(k, par, i, j).wait_send()
        for which in range(tokens // rows):
            @pl.when(jnp.logical_not(jnp.logical_and(i == a, which == t)))
            def _():
                o_copy(i, which).wait_send()
    for e in range(2):
        for dy in range(1, chips):
            wo_y(dy, e).wait_send()
        for dy in range(chips):
            wo_c(dy, e).wait_send()
    row_z().wait_send()
    for r in range(peers):
        row_near(r).wait_send()
        for h in range(plan.halves):
            half_near(h, r).wait_send()
        if r % chips:
            row_y(r // chips, r % chips).wait_send()
            for h in range(plan.halves):
                sum_y(h, r // chips, r % chips).wait_send()
    for h in range(plan.halves):
        sum_z(h).wait_send()


def run_layer(plan, lams, small, large, gain, outs, residual, norm_gain, mixer, width):
    dma = pltpu.SemaphoreType.DMA
    slots, n, m, peers, chips = plan.slots, plan.n, plan.m, plan.peers, plan.chips
    rows, features, units, halves = plan.rows, plan.features, plan.sizes[0], plan.halves
    high, pieces = plan.high, len(plan.pieces)
    anywhere = pl.BlockSpec(memory_space=pl.ANY)
    vmem = pl.BlockSpec(memory_space=pltpu.VMEM)
    smem = pl.BlockSpec(memory_space=pltpu.SMEM)
    others, ahead = max(plan.group - 1, 1), max(chips - 1, 1)
    bf16, f32 = jnp.bfloat16, jnp.float32
    return pl.pallas_call(
        functools.partial(layer_kernel, plan),
        out_shape=jax.ShapeDtypeStruct((rows, features), bf16),
        in_specs=[smem] * 2 + [anywhere] * 6 + [vmem] + [anywhere] * 2 + [vmem] * 2 + [anywhere] * 3,
        out_specs=vmem,
        scratch_shapes=[
            pltpu.VMEM((3, n * plan.tokens, width), bf16),
            pltpu.VMEM((2, slots, plan.tokens, width), bf16),
            pltpu.VMEM((slots, plan.tokens, width), bf16),
            pltpu.VMEM((m * slots, rows, width), bf16),
            pltpu.VMEM((2, high, n * plan.tokens), f32),
            pltpu.VMEM((2, high, 128), f32),
            pltpu.VMEM((2, high, 128), f32),
            pltpu.VMEM((2, high, width), f32),
            pltpu.VMEM((m, slots * width, features), bf16),
            pltpu.VMEM((features, units), bf16),
            pltpu.VMEM((features, units), bf16),
            pltpu.VMEM((halves, units, features // halves), bf16),
            pltpu.VMEM((peers, 2, rows, features), bf16),
            pltpu.VMEM((peers, 2 * rows, units), bf16),
        ] + [pltpu.VMEM((halves, peers, rows, features // halves), bf16)] * 4 + [
            dma((slots,)), dma((slots,)), dma((slots,)), dma((slots,)), dma((slots,)), dma((slots,)),
            dma((slots, others)), dma((slots, others)), dma((slots, others)), dma((slots, others)),
            dma((5,)),
            dma((slots, plan.tokens // rows)), dma((m * slots,)),
            dma((pieces, slots)), dma((pieces, slots)),
            dma((pieces, slots, others)), dma((pieces, slots, others)),
            dma((pieces,)),
            dma((ahead, 2)), dma((ahead, 2)), dma((chips, 2)), dma((chips, 2)),
            dma((peers,)), dma((peers,)), dma((peers,)), dma((peers,)),
            dma((halves, peers)), dma((halves, peers)), dma((halves, peers)), dma((halves, peers)),
        ],
        compiler_params=pltpu.CompilerParams(
            vmem_limit_bytes=61 * 2**20, has_side_effects=True, collective_id=0),
        cost_estimate=pl.CostEstimate(
            flops=60_000_000_000, bytes_accessed=16_000_000, transcendentals=8_000_000),
        name="layer",
    )(*lams, *small, *large, gain.reshape(1, width), *outs, residual, norm_gain.reshape(1, features), *mixer)


def per_device(
    residual, query_small, key_small, value_small, query_large, key_large, value_large,
    lambda_small, lambda_large, head_gain, output_small, output_large, norm_gain,
    gate_weight, up_weight, down_weight,
):
    tokens, heads_small, width = value_small.shape
    heads_large = value_large.shape[1]
    rows, features = residual.shape
    n, m = lax.axis_size("sp"), lax.axis_size("tp")
    short = -gate_weight.shape[1] % 128
    if short:
        gate_weight = jnp.pad(gate_weight, ((0, 0), (0, short)))
        up_weight = jnp.pad(up_weight, ((0, 0), (0, short)))
        down_weight = jnp.pad(down_weight, ((0, short), (0, 0)))
    plan = Plan(n, m, heads_small, heads_large, tokens, rows, query_small.shape[2] // 2,
                query_large.shape[2] // 2, features, gate_weight.shape[1])

    def by_head(values):
        parts = values.reshape(tokens, values.shape[1], -1, width)
        return jnp.transpose(parts, (1, 2, 0, 3))

    small = [by_head(v) for v in (key_small, value_small, query_small)]
    large = [by_head(v) for v in (key_large, value_large, query_large)]
    return run_layer(
        plan, (lambda_small, lambda_large), small, large, head_gain, (output_small, output_large),
        residual, norm_gain, (gate_weight, up_weight, down_weight), width)


def solution(mesh):
    in_specs = (
        P(("sp", "tp"), None), P("sp", "tp", None), P("sp", "tp", None), P("sp", "tp", None),
        P("sp", "tp", None), P("sp", "tp", None), P("sp", "tp", None), P("tp"), P("tp"), P(),
        P("tp", None), P("tp", None), P(), P("sp", "tp"), P("sp", "tp"), P("tp", "sp"),
    )

    return jax.shard_map(per_device, mesh=mesh, in_specs=in_specs, out_specs=P(("sp", "tp"), None), check_vma=False)
```

```python
import functools

import jax
import jax.numpy as jnp
from jax import lax
from jax.experimental import pallas as pl
from jax.experimental.pallas import tpu as pltpu
from jax.sharding import PartitionSpec as P

residual_scale = 8.0**0.25
branch_scale = 0.8
norm_epsilon = 1e-05
masked_score = -1e30
log2_e = 1.4426950408889634
MESH = pl.DeviceIdType.MESH


def layer_norm(values, gains):
    centered = values - jnp.mean(values, axis=-1, keepdims=True)
    variance = jnp.mean(centered * centered, axis=-1, keepdims=True)
    return centered * lax.rsqrt(variance + norm_epsilon) * gains


def fold_lanes(values, op):
    result = values[:, :128]
    for start in range(128, values.shape[1], 128):
        result = op(result, values[:, start : start + 128])
    return result


class Plan:
    def __init__(self, n, m, small, large, tokens, rows, small_size, large_size, features, units):
        self.n, self.m, self.chips, self.peers = n, m, m // 2, m
        self.slots = small + large
        self.group = n // self.slots
        half = small // 2
        self.kinds = [("s", i) for i in range(half)]
        self.kinds += [("l", i) for i in range(large)]
        self.kinds += [("s", i) for i in range(half, small)]
        self.keys = [1 if kind == "s" else 2 for kind, _ in self.kinds]
        self.natural = [self.kinds.index(("s", i)) for i in range(small)]
        self.natural += [self.kinds.index(("l", i)) for i in range(large)]
        self.tokens, self.rows, self.features = tokens, rows, features
        self.small_size, self.large_size = small_size, large_size
        tiles = units // 128
        first = (tiles + 1) // 2 * 128
        self.sizes, self.offsets = (units - first, first), (0, units - first)
        self.half_of = [(i + 1) // 2 % 2 for i in range(self.slots)]
        self.depth = features // n
        self.halves = max(1, self.depth // 128)
        self.span = self.depth // self.halves
        self.columns = [(start, tuple(max(0, min(256, size - start)) for size in self.sizes))
                        for start in range(0, first, 256)]
        self.pieces = [(tensor, j) for j in range(len(self.columns)) for tensor in (0, 1)]
        self.ups = len(self.pieces)
        self.pieces += [(2, (h, part)) for h in range(self.halves) for part in range(2)]
        keys = n * tokens
        self.high = tokens
        while self.high > 128 and self.high * keys > 2**21:
            self.high //= 2


def layer_kernel(plan, lam_small, lam_large, k_small_in, v_small_in, q_small_in, k_large_in, v_large_in,
                 q_large_in, gain_ref,
                 out_small, out_large, residual_ref, norm_ref, gate, up, down, out_ref,
                 k_small, v_small, q_small, k_large, v_large, q_large, kv, q, o, att, pool, peak, total, acc, w_out, w_gate, w_up, w_down, x, hidden,
                 kz_s, kz_r, vz_s, vz_r, qz_s, qz_r, kx_s, kx_r, vx_s, vx_r, loc, o_s, o_r,
                 wz_s, wz_r, wx_s, wx_r, own_w, wy_s, wy_r, wc_s, wc_r,
                 ag_s, ag_r, agc_s, agc_r, rc_s, rc_r,
                 ya_s, ya_r, zb_s, zb_r, za_s, za_r, yb_s, yb_r):
    slots, group, m, n = plan.slots, plan.group, plan.m, plan.n
    tokens, rows, chips, depth = plan.tokens, plan.rows, plan.chips, plan.depth
    features = plan.features
    s = lax.axis_index("sp")
    t = lax.axis_index("tp")
    a, b = s // group, lax.rem(s, group)
    y, c = t // 2, lax.rem(t, 2)
    parity = lax.rem(a, 2)
    partner = y * 2 + 1 - c
    aside = lax.rem(s + 1, n)
    mine = pl.ds(pl.multiple_of(s * tokens, tokens), tokens)
    large = a < 0
    for i, k in enumerate(plan.keys):
        if k == 2:
            large = jnp.logical_or(large, a == i)
    by_kind = ((1, jnp.logical_not(large)), (2, large))
    share = lax.rem((a + 1) // 2, 2)
    by_parity = ((0, share == 0), (1, share == 1))

    def remote(src, dst, send, recv, sp, tp):
        return pltpu.make_async_remote_copy(
            src_ref=src, dst_ref=dst, send_sem=send, recv_sem=recv,
            device_id={"sp": sp, "tp": tp}, device_id_type=MESH)

    def arrival(dst, recv):
        remote(dst, dst, kz_s.at[0], recv, aside, t).wait_recv()

    def block_of(i):
        return pl.ds(pl.multiple_of((i * group + b) * tokens, tokens), tokens)

    def source(i, what):
        kind, index = plan.kinds[i]
        return {"s": (k_small, v_small, q_small), "l": (k_large, v_large, q_large)}[kind][what].at[index]

    def to_slot(i, what):
        keys = pl.ds(0, plan.keys[i])
        dst = (kv.at[keys, mine], kv.at[pl.ds(2, 1), mine], q.at[keys, a])[what]
        send, recv = ((kz_s, kz_r), (vz_s, vz_r), (qz_s, qz_r))[what]
        return remote(source(i, what), dst, send.at[i], recv.at[a], i * group + b, t)

    def keep(i, what):
        keys = pl.ds(0, plan.keys[i])
        if what == 0:
            kv[keys, mine] = source(i, what)[...]
        elif what == 1:
            kv[pl.ds(2, 1), mine] = source(i, what)[...]
        else:
            q[keys, a] = source(i, what)[...]

    def by_head(values, out):
        width = out.shape[3]
        for part in range(out.shape[1]):
            piece = values[:, :, part * width : (part + 1) * width]
            out[:, part] = jnp.transpose(piece, (1, 0, 2))

    def peer(j):
        return a * group + lax.rem(b + j, group)

    def k_x(k, i, j):
        part = kv.at[pl.ds(0, k), block_of(i)]
        return remote(part, part, kx_s.at[i, j - 1], kx_r.at[i, j - 1], peer(j), t)

    def k_own(i, j):
        keys = pl.ds(0, plan.keys[i])
        return remote(source(i, 0), kv.at[keys, mine], kx_s.at[i, j - 1], kx_r.at[i, j - 1], peer(j), t)

    def v_own(i, j):
        return remote(source(i, 1), kv.at[pl.ds(2, 1), mine], vx_s.at[i, j - 1], vx_r.at[i, j - 1], peer(j), t)

    def v_x(i, j):
        part = kv.at[pl.ds(2, 1), block_of(i)]
        return remote(part, part, vx_s.at[i, j - 1], vx_r.at[i, j - 1], peer(j), t)

    pieces = len(plan.pieces)

    def piece_in(k, par):
        tensor, which = plan.pieces[k]
        if tensor < 2:
            start, widths = plan.columns[which]
            return (gate, up)[tensor].at[:, pl.ds(plan.offsets[par] + start, widths[par])]
        h, part = which
        size = plan.sizes[par] // 2
        return down.at[pl.ds(plan.offsets[par] + part * size, size), pl.ds(h * plan.span, plan.span)]

    def piece_at(k, par, block):
        tensor, which = plan.pieces[k]
        if tensor < 2:
            start, widths = plan.columns[which]
            return (w_gate, w_up)[tensor].at[
                pl.ds(pl.multiple_of(block * depth, depth), depth), pl.ds(start, widths[par])]
        h, part = which
        size = plan.sizes[par] // 2
        return w_down.at[h, pl.ds(part * size, size),
                         pl.ds(pl.multiple_of(block * plan.span, plan.span), plan.span)]

    def w_z(k, i):
        return remote(piece_in(k, plan.half_of[i]), piece_at(k, plan.half_of[i], s), wz_s.at[k, i], wz_r.at[k, a],
                      i * group + b, t)

    def w_own(k, par):
        return pltpu.make_async_copy(piece_in(k, par), piece_at(k, par, s), own_w.at[k])

    def w_x(k, par, i, j):
        part = piece_at(k, par, i * group + b)
        return remote(part, part, wx_s.at[k, i, j - 1], wx_r.at[k, i, j - 1], peer(j), t)

    def w_near(k):
        for i in range(slots):
            @pl.when(i == a + 1 - 2 * parity)
            def _():
                w_z(k, i).start()

    def w_far(k):
        for distance in range(1, slots):
            for i in range(slots):
                @pl.when(jnp.logical_and(jnp.abs(a - i) == distance, i != a + 1 - 2 * parity))
                def _():
                    w_z(k, i).start()

    def w_share(k):
        for par, when in by_parity:
            @pl.when(when)
            def _():
                w_own(k, par).wait()
                for i in range(slots):
                    @pl.when(a == i)
                    def _():
                        for j in range(1, group):
                            w_x(k, par, i, j).start()

    def w_pass(k, par, i):
        arrival(piece_at(k, par, i * group + b), wz_r.at[k, i])
        for j in range(1, group):
            w_x(k, par, i, j).start()

    def pass_near(k):
        for i in range(slots):
            @pl.when(i == a + 1 - 2 * parity)
            def _():
                w_pass(k, plan.half_of[i ^ 1], i)

    def pass_far(k):
        for par, when in by_parity:
            @pl.when(when)
            def _():
                for distance in range(1, slots):
                    for i in range(slots):
                        @pl.when(jnp.logical_and(jnp.abs(a - i) == distance, i != a + 1 - 2 * parity))
                        def _():
                            w_pass(k, par, i)

    def w_forward(k):
        pass_near(k)
        pass_far(k)

    def w_wait(k):
        for par, when in by_parity:
            @pl.when(when)
            def _():
                for i in range(slots):
                    for j in range(1, group):
                        block = i * group + lax.rem(b + group - j, group)
                        arrival(piece_at(k, par, block), wx_r.at[k, i, j - 1])

    def tp_of(dy):
        return lax.rem(y + dy, chips) * 2 + c

    cut = out_small.shape[0]
    deep = cut + out_large.shape[0]
    spans = ((out_small, 0, cut), (out_large, cut, out_large.shape[0]))

    def wo_at(tp, e):
        return w_out.at[pl.ds(pl.multiple_of(tp * deep + spans[e][1], 128), spans[e][2])]

    def stash(which, h, r, start, size):
        low = features // plan.halves
        return w_out.at[pl.ds((which * m + r) * rows, rows), pl.ds(h * low + start, size)]


    def wo_y(dy, e):
        part = spans[e][0]
        return remote(part, wo_at(t, e), wy_s.at[dy - 1, e], wy_r.at[chips - dy - 1, e], s, tp_of(dy))

    def wo_c(dy, e):
        part = spans[e][0]
        there = wo_at(tp_of(dy), e)
        return remote(part if dy == 0 else there, there, wc_s.at[dy, e], wc_r.at[dy, e], s, partner)

    def wo_own(e):
        return pltpu.make_async_copy(spans[e][0], wo_at(t, e), loc.at[e])

    pair = (a + 1 - 2 * parity) * group + b

    def row_z():
        return remote(x.at[0, 0], x.at[chips, 0], ag_s.at[0], ag_r.at[chips], pair, t)

    def row_y(dz, dy):
        r = dz * chips + dy
        into = dz * chips + chips - dy
        return remote(x.at[dz * chips, 0], x.at[into, 0], ag_s.at[r], ag_r.at[into], s, tp_of(dy))

    def row_near(r):
        return remote(x.at[r, 0], x.at[r, 1], agc_s.at[r], agc_r.at[r], s, partner)

    side = features // plan.halves // 2

    def half_near(h, r):
        return remote(stash(0, h, r, 0, 2 * side), stash(1, h, r, 0, 2 * side), rc_s.at[h, r], rc_r.at[h, r], s, partner)

    by_y, by_z = (0, side), (side, side)

    def y_first(h, dz, dy):
        r, into = dz * chips + dy, dz * chips + chips - dy
        return remote(stash(2, h, r, *by_y), stash(3, h, into, *by_y),
                      ya_s.at[h, r], ya_r.at[h, into], s, tp_of(dy))

    def z_second(h):
        return remote(stash(2, h, chips, *by_y), stash(3, h, 0, *by_y),
                      zb_s.at[h], zb_r.at[h], pair, t)

    def z_first(h, dy):
        return remote(stash(2, h, chips + dy, *by_z), stash(3, h, chips + dy, *by_z),
                      za_s.at[h, dy], za_r.at[h, dy], pair, t)

    def y_second(h, dy):
        return remote(stash(2, h, dy, *by_z), stash(3, h, chips - dy, *by_z),
                      yb_s.at[h, dy], yb_r.at[h, chips - dy], s, tp_of(dy))

    barrier = pltpu.get_barrier_semaphore()
    for i in range(slots):
        for tt in range(m):
            @pl.when(jnp.logical_not(jnp.logical_and(i == a, tt == t)))
            def _():
                pl.semaphore_signal(barrier, inc=1, device_id={"sp": i * group + b, "tp": tt},
                                    device_id_type=MESH)
    for j in range(1, group):
        pl.semaphore_signal(barrier, inc=1, device_id={"sp": peer(j), "tp": t}, device_id_type=MESH)
    by_head(k_large_in, k_large)
    by_head(k_small_in, k_small)
    for e in range(2):
        wo_own(e).start()
    for par, when in by_parity:
        @pl.when(when)
        def _():
            for k in range(pieces):
                w_own(k, par).start()
    by_head(v_large_in, v_large)
    by_head(v_small_in, v_small)
    pl.semaphore_wait(barrier, slots * m - 1 + group - 1)

    for what in range(3):
        for distance in range(1, slots):
            for i in range(slots):
                @pl.when(jnp.abs(a - i) == distance)
                def _():
                    to_slot(i, what).start()
        if what == 1:
            by_head(q_large_in, q_large)
            by_head(q_small_in, q_small)
    for e in range(2):
        for dy in range(1, chips):
            wo_y(dy, e).start()
        wo_c(0, e).start()
    spare_units = plan.sizes[1] - plan.sizes[0]
    if spare_units:
        @pl.when(share == 0)
        def _():
            spare = pl.ds(plan.sizes[0], spare_units)
            w_gate[:, spare] = jnp.zeros((features, spare_units), w_gate.dtype)
            w_up[:, spare] = jnp.zeros((features, spare_units), w_up.dtype)
            for h in range(plan.halves):
                w_down[h, spare, :] = jnp.zeros((spare_units, features // plan.halves), w_down.dtype)

    for i in range(slots):
        @pl.when(a == i)
        def _():
            for what in range(3):
                keep(i, what)
            for j in range(1, group):
                k_own(i, j).start()
                v_own(i, j).start()

    for distance in range(1, slots):
        for i in range(slots):
            for k, when in by_kind:
                @pl.when(jnp.logical_and(when, jnp.abs(a - i) == distance))
                def _():
                    arrival(kv.at[pl.ds(0, k), block_of(i)], kz_r.at[i])
                    for j in range(1, group):
                        k_x(k, i, j).start()
    for distance in range(1, slots):
        for i in range(slots):
            @pl.when(jnp.abs(a - i) == distance)
            def _():
                arrival(kv.at[pl.ds(2, 1), block_of(i)], vz_r.at[i])
                for j in range(1, group):
                    v_x(i, j).start()

    w_near(0)
    w_far(0)
    for k in range(pieces):
        w_share(k)

    def ready(i):
        for k, when in by_kind:
            @pl.when(when)
            def _():
                @pl.when(a != i)
                def _():
                    arrival(q.at[pl.ds(0, k), i], qz_r.at[i])

                for j in range(1, group):
                    block = i * group + lax.rem(b + group - j, group)
                    from_peer = pl.ds(pl.multiple_of(block * tokens, tokens), tokens)
                    arrival(kv.at[pl.ds(0, k), from_peer], kx_r.at[i, j - 1])
                    arrival(kv.at[pl.ds(2, 1), from_peer], vx_r.at[i, j - 1])

        @pl.when(jnp.logical_not(large))
        def _():
            both = q[0, i]
            lane = lax.broadcasted_iota(jnp.int32, both.shape, 1)
            q[1, i] = jnp.where(lane >= plan.small_size, both, jnp.zeros_like(both))
            q[0, i] = jnp.where(lane < plan.small_size, both, jnp.zeros_like(both))

    lift = large.astype(jnp.int32)
    factor = jnp.where(large, plan.large_size**-0.5 * log2_e, plan.small_size**-0.5 * log2_e)
    lam = jnp.float32(0.0)
    for i, (kind, index) in enumerate(plan.kinds):
        lam = jnp.where(a == i, (lam_small if kind == "s" else lam_large)[index], lam)
    last = (((1,), (1,)), ((), ()))
    high = plan.high
    parts = tokens // high
    wide = group * tokens
    strip = min(512, tokens)
    head = t * slots + a

    def o_copy(i, which):
        return remote(o.at[i, pl.ds(pl.multiple_of(which * rows, rows), rows)], att.at[head],
                      o_s.at[i, which], o_r.at[head], i * group + b, which)

    def attend(i, part):
        row0 = part * high
        here = pl.ds(pl.multiple_of(row0, high), high)
        queries = (q[0, i, here], q[1, i, here])

        def find(chunk, last_one):
            for which in range(2):
                for off in range(0, wide, strip):
                    at = pl.ds(pl.multiple_of(chunk * wide + off, strip), strip)
                    score = lax.dot_general(
                        queries[which], kv[which * lift, at], last, preferred_element_type=jnp.float32)
                    if last_one:
                        row = b * tokens + row0 + lax.broadcasted_iota(jnp.int32, score.shape, 0)
                        column = off + lax.broadcasted_iota(jnp.int32, score.shape, 1)
                        score = jnp.where(column <= row, score, masked_score)
                    pool[which, :, at] = score
                    top = fold_lanes(score, jnp.maximum)
                    fresh = last_one and off == 0
                    peak[which] = top if fresh else jnp.maximum(peak[which], top)

        find(i, True)
        lax.fori_loop(0, i, lambda chunk, carry: find(chunk, False) or carry, 0)
        for which in range(2):
            peak[which] = jnp.broadcast_to(
                jnp.max(peak[which], axis=1, keepdims=True), (high, 128))

        def weigh(chunk, fresh):
            for which in range(2):
                sums = outs = None
                for off in range(0, wide, strip):
                    at = pl.ds(pl.multiple_of(chunk * wide + off, strip), strip)
                    score = pool[which, :, at]
                    top = peak[which]
                    weights = jnp.concatenate(
                        [jnp.exp2((score[:, u : u + 128] - top) * factor) for u in range(0, strip, 128)],
                        axis=1)
                    part_sum = fold_lanes(weights, jnp.add)
                    part_out = jnp.dot(
                        weights.astype(jnp.bfloat16), kv[2, at], preferred_element_type=jnp.float32)
                    sums = part_sum if sums is None else sums + part_sum
                    outs = part_out if outs is None else outs + part_out
                if fresh:
                    total[which], acc[which] = sums, outs
                else:
                    total[which] += sums
                    acc[which] += outs

        weigh(i, True)
        lax.fori_loop(0, i, lambda chunk, carry: weigh(chunk, False) or carry, 0)
        outs = [acc[which] / jnp.sum(total[which], axis=1, keepdims=True) for which in range(2)]
        combined = outs[0] - lam * outs[1]
        mean_square = jnp.mean(combined * combined, axis=1, keepdims=True)
        normed = combined * lax.rsqrt(mean_square + norm_epsilon) * gain_ref[...] * branch_scale
        o[i, here] = normed.astype(o.dtype)

    def send(i):
        for which in range(tokens // rows):
            @pl.when(jnp.logical_not(jnp.logical_and(i == a, which == t)))
            def _():
                o_copy(i, which).start()

    def wo_forward():
        for dy in range(1, chips):
            for e in range(2):
                arrival(wo_at(tp_of(dy), e), wy_r.at[dy - 1, e])
                wo_c(dy, e).start()

    def step_body(i, carry):
        for at in range(slots):
            @pl.when(i == at)
            def _():
                ready(at)
                if at == slots // 2 - 1:
                    for k in (1, 2):
                        w_near(k)
                        w_far(k)
                if at == slots // 2:
                    for k in range(3, pieces):
                        w_near(k)
        lax.fori_loop(0, parts, lambda part, c: attend(i, part) or c, 0)

        @pl.when(i > 0)
        def _():
            send(i - 1)

        return carry

    lax.fori_loop(0, slots, step_body, 0)
    att[head] = o[a, pl.ds(pl.multiple_of(t * rows, rows), rows)]
    send(slots - 1)
    w_far(3)
    w_forward(0)
    wo_forward()
    w_forward(1)

    for e in range(2):
        wo_own(e).wait()
        for dy in range(chips):
            block = lax.rem(y + dy, chips) * 2 + 1 - c
            arrival(wo_at(block, e), wc_r.at[dy, e])
    for h in range(m * slots):
        @pl.when(head != h)
        def _():
            arrival(att.at[h], o_r.at[h])
    for e in range(2):
        for dy in range(chips):
            wo_c(dy, e).wait_send()
    stretch = 512
    base = plan.features
    for start in range(0, features, stretch):
        cols = pl.ds(start, stretch)
        sums = None
        for tt in range(m):
            left = jnp.concatenate([att[tt * slots + i] for i in plan.natural], axis=1)
            term = jnp.dot(left, w_out[pl.ds(tt * deep, deep), cols], preferred_element_type=jnp.float32)
            sums = term if sums is None else sums + term
        pool[1, pl.ds(0, rows), pl.ds(base + start, stretch)] = (
            residual_scale * residual_ref[:, cols].astype(jnp.float32) + sums)
    x[0, 0] = layer_norm(pool[1, pl.ds(0, rows), pl.ds(base, features)], norm_ref[...]).astype(x.dtype)
    peers = plan.peers
    row_z().start()
    for dy in range(1, chips):
        row_y(0, dy).start()
    row_near(0).start()
    for k in range(4, pieces):
        w_far(k)

    def gate_up(j, lo, hi):
        start, widths = plan.columns[j]
        cols = pl.ds(start, max(widths))

        def one(r, carry):
            both = x[r].reshape(2 * rows, features)
            g = jnp.dot(both, w_gate[:, cols], preferred_element_type=jnp.float32)
            u = jnp.dot(both, w_up[:, cols], preferred_element_type=jnp.float32)
            hidden[r, :, cols] = (g / (1.0 + jnp.exp(-g)) * u).astype(hidden.dtype)
            return carry

        lax.fori_loop(lo, hi, one, 0)

    def forward_to(last):
        for k in range(state["done"], min(last, pieces)):
            if k < 3:
                pass_near(k)
            pass_far(k)
            state["done"] = k + 1

    def rows_y(dz):
        for dy in range(1, chips):
            r = dz * chips + dy
            arrival(x.at[r, 0], ag_r.at[r])
            row_near(r).start()

    def rows_near(dz):
        for r in range(dz * chips, dz * chips + chips):
            arrival(x.at[r, 1], agc_r.at[r])

    def columns_here(j):
        w_wait(2 * j)
        w_wait(2 * j + 1)

    state = {"done": 2}
    ups = plan.ups
    early = len(plan.columns) - 1
    forward_to(3)
    for k in range(3, pieces):
        pass_near(k)
    forward_to(4)
    rows_y(0)
    forward_to(5)
    arrival(x.at[chips, 0], ag_r.at[chips])
    for dy in range(1, chips):
        row_y(1, dy).start()
    row_near(chips).start()
    rows_near(0)
    for j in range(early):
        forward_to(2 * j + 2)
        columns_here(j)
        gate_up(j, 0, chips)
    forward_to(ups)
    rows_y(1)
    forward_to(ups + 1)
    rows_near(1)
    gate_up(0, chips, peers)
    forward_to(ups + 2)
    if early > 1:
        gate_up(1, chips, peers)
    forward_to(ups + 3)
    for j in range(2, early):
        gate_up(j, chips, peers)
    columns_here(early)
    gate_up(early, 0, peers)
    forward_to(ups + 4)

    low = features // plan.halves
    band = min(512, low)
    per_plane = high // rows

    def kept(r, cols):
        return pool.at[r // per_plane, pl.ds(r % per_plane * rows, rows), cols]

    def down_rows(h, r):
        for start in range(0, low, band):
            cols = pl.ds(start, band)
            part = jnp.dot(hidden[r], w_down[h, :, cols], preferred_element_type=jnp.float32)
            kept(r, pl.ds(h * low + start, band))[...] = part[:rows]
            stash(0, h, r, start, band)[...] = part[rows:].astype(w_out.dtype)

    def chip_sum(h, r, which):
        cols = pl.ds(h * low + which * side, side)
        return kept(r, cols)[...] + stash(1, h, r, which * side, side)[...].astype(jnp.float32)

    def down_half(h):
        order = [chips + dy for dy in range(1, chips)] + [chips] + list(range(1, chips)) + [0]

        def pass_on(r):
            dz, dy = r // chips, r % chips
            arrival(stash(1, h, r, 0, 2 * side), rc_r.at[h, r])
            if dy:
                stash(2, h, r, *by_y)[...] = chip_sum(h, r, 0).astype(w_out.dtype)
                y_first(h, dz, dy).start()
            if dz:
                stash(2, h, r, *by_z)[...] = chip_sum(h, r, 1).astype(w_out.dtype)
                z_first(h, dy).start()

        for place, r in enumerate(order):
            down_rows(h, r)
            half_near(h, r).start()
            if place:
                pass_on(order[place - 1])
        pass_on(0)

    def plane_sum(h, dz):
        result = chip_sum(h, dz * chips, 0)
        for dy in range(1, chips):
            r = dz * chips + dy
            arrival(stash(3, h, r, *by_y), ya_r.at[h, r])
            result += stash(3, h, r, *by_y)[...].astype(jnp.float32)
        return result

    def line_sum(h, dy):
        arrival(stash(3, h, chips + dy, *by_z), za_r.at[h, dy])
        return chip_sum(h, dy, 1) + stash(3, h, chips + dy, *by_z)[...].astype(jnp.float32)

    def second_sums(h):
        stash(2, h, chips, *by_y)[...] = plane_sum(h, 1).astype(w_out.dtype)
        z_second(h).start()
        for dy in range(1, chips):
            stash(2, h, dy, *by_z)[...] = line_sum(h, dy).astype(w_out.dtype)
            y_second(h, dy).start()

    def finish(h):
        first = plane_sum(h, 0)
        arrival(stash(3, h, 0, *by_y), zb_r.at[h])
        first += stash(3, h, 0, *by_y)[...].astype(jnp.float32)
        second = line_sum(h, 0)
        for dy in range(1, chips):
            arrival(stash(3, h, dy, *by_z), yb_r.at[h, dy])
            second += stash(3, h, dy, *by_z)[...].astype(jnp.float32)
        result = jnp.concatenate([first, second], axis=1)
        for block in range(n):
            cols = pl.ds(block * depth + h * plan.span, plan.span)
            out_ref[:, cols] = (
                residual_scale * x[0, 0, :, cols].astype(jnp.float32)
                + 0.5 * result[:, block * plan.span : (block + 1) * plan.span]
            ).astype(out_ref.dtype)

    for h in range(plan.halves):
        first = plan.ups + 2 * h
        forward_to(first + 2)
        w_wait(first)
        w_wait(first + 1)
        down_half(h)
        if h:
            second_sums(h - 1)
    second_sums(plan.halves - 1)
    for h in range(plan.halves):
        finish(h)

    for i in range(slots):
        @pl.when(a != i)
        def _():
            for what in range(3):
                to_slot(i, what).wait_send()
            for k in range(pieces):
                w_z(k, i).wait_send()

        for k, when in by_kind:
            @pl.when(when)
            def _():
                for j in range(1, group):
                    k_x(k, i, j).wait_send()
                    v_x(i, j).wait_send()
        for par, when in by_parity:
            @pl.when(when)
            def _():
                for j in range(1, group):
                    for k in range(pieces):
                        w_x(k, par, i, j).wait_send()
        for which in range(tokens // rows):
            @pl.when(jnp.logical_not(jnp.logical_and(i == a, which == t)))
            def _():
                o_copy(i, which).wait_send()
    for e in range(2):
        for dy in range(1, chips):
            wo_y(dy, e).wait_send()
    row_z().wait_send()
    for r in range(peers):
        row_near(r).wait_send()
        for h in range(plan.halves):
            half_near(h, r).wait_send()
            if r % chips:
                y_first(h, r // chips, r % chips).wait_send()
        if r % chips:
            row_y(r // chips, r % chips).wait_send()
    for h in range(plan.halves):
        z_second(h).wait_send()
        for dy in range(chips):
            z_first(h, dy).wait_send()
            if dy:
                y_second(h, dy).wait_send()


def run_layer(plan, lams, small, large, gain, outs, residual, norm_gain, mixer, width):
    dma = pltpu.SemaphoreType.DMA
    slots, n, m, peers, chips = plan.slots, plan.n, plan.m, plan.peers, plan.chips
    rows, features, units, halves = plan.rows, plan.features, plan.sizes[1], plan.halves
    high, pieces = plan.high, len(plan.pieces)
    anywhere = pl.BlockSpec(memory_space=pl.ANY)
    vmem = pl.BlockSpec(memory_space=pltpu.VMEM)
    smem = pl.BlockSpec(memory_space=pltpu.SMEM)
    others, ahead = max(plan.group - 1, 1), max(chips - 1, 1)
    bf16, f32 = jnp.bfloat16, jnp.float32
    return pl.pallas_call(
        functools.partial(layer_kernel, plan),
        out_shape=jax.ShapeDtypeStruct((rows, features), bf16),
        in_specs=[smem] * 2 + [vmem] * 7 + [anywhere] * 2 + [vmem] * 2 + [anywhere] * 3,
        out_specs=vmem,
        scratch_shapes=[
            pltpu.VMEM((small[0].shape[1], 1, plan.tokens, width), bf16),
            pltpu.VMEM((small[0].shape[1], 1, plan.tokens, width), bf16),
            pltpu.VMEM((small[0].shape[1], 1, plan.tokens, width), bf16),
            pltpu.VMEM((large[0].shape[1], 2, plan.tokens, width), bf16),
            pltpu.VMEM((large[0].shape[1], 1, plan.tokens, width), bf16),
            pltpu.VMEM((large[0].shape[1], 2, plan.tokens, width), bf16),
            pltpu.VMEM((3, n * plan.tokens, width), bf16),
            pltpu.VMEM((2, slots, plan.tokens, width), bf16),
            pltpu.VMEM((slots, plan.tokens, width), bf16),
            pltpu.VMEM((m * slots, rows, width), bf16),
            pltpu.VMEM((2, high, n * plan.tokens), f32),
            pltpu.VMEM((2, high, 128), f32),
            pltpu.VMEM((2, high, 128), f32),
            pltpu.VMEM((2, high, width), f32),
            pltpu.VMEM((max(m * slots * width, 4 * m * rows), features), bf16),
            pltpu.VMEM((features, units), bf16),
            pltpu.VMEM((features, units), bf16),
            pltpu.VMEM((halves, units, features // halves), bf16),
            pltpu.VMEM((peers, 2, rows, features), bf16),
            pltpu.VMEM((peers, 2 * rows, units), bf16),
            dma((slots,)), dma((slots,)), dma((slots,)), dma((slots,)), dma((slots,)), dma((slots,)),
            dma((slots, others)), dma((slots, others)), dma((slots, others)), dma((slots, others)),
            dma((2,)),
            dma((slots, plan.tokens // rows)), dma((m * slots,)),
            dma((pieces, slots)), dma((pieces, slots)),
            dma((pieces, slots, others)), dma((pieces, slots, others)),
            dma((pieces,)),
            dma((ahead, 2)), dma((ahead, 2)), dma((chips, 2)), dma((chips, 2)),
            dma((peers,)), dma((peers,)), dma((peers,)), dma((peers,)),
            dma((halves, peers)), dma((halves, peers)),
            dma((halves, peers)), dma((halves, peers)), dma((halves,)), dma((halves,)),
            dma((halves, chips)), dma((halves, chips)), dma((halves, chips)), dma((halves, chips)),
        ],
        compiler_params=pltpu.CompilerParams(
            vmem_limit_bytes=61 * 2**20, has_side_effects=True, collective_id=0),
        cost_estimate=pl.CostEstimate(
            flops=60_000_000_000, bytes_accessed=16_000_000, transcendentals=8_000_000),
        name="layer",
    )(*lams, *small, *large, gain.reshape(1, width), *outs, residual, norm_gain.reshape(1, features), *mixer)


def per_device(
    residual, query_small, key_small, value_small, query_large, key_large, value_large,
    lambda_small, lambda_large, head_gain, output_small, output_large, norm_gain,
    gate_weight, up_weight, down_weight,
):
    tokens, heads_small, width = value_small.shape
    heads_large = value_large.shape[1]
    rows, features = residual.shape
    n, m = lax.axis_size("sp"), lax.axis_size("tp")
    short = -gate_weight.shape[1] % 128
    if short:
        gate_weight = jnp.pad(gate_weight, ((0, 0), (0, short)))
        up_weight = jnp.pad(up_weight, ((0, 0), (0, short)))
        down_weight = jnp.pad(down_weight, ((0, short), (0, 0)))
    plan = Plan(n, m, heads_small, heads_large, tokens, rows, query_small.shape[2] // 2,
                query_large.shape[2] // 2, features, gate_weight.shape[1])

    small = (key_small, value_small, query_small)
    large = (key_large, value_large, query_large)
    return run_layer(
        plan, (lambda_small, lambda_large), small, large, head_gain, (output_small, output_large),
        residual, norm_gain, (gate_weight, up_weight, down_weight), width)


def solution(mesh):
    in_specs = (
        P(("sp", "tp"), None), P("sp", "tp", None), P("sp", "tp", None), P("sp", "tp", None),
        P("sp", "tp", None), P("sp", "tp", None), P("sp", "tp", None), P("tp"), P("tp"), P(),
        P("tp", None), P("tp", None), P(), P("sp", "tp"), P("sp", "tp"), P("tp", "sp"),
    )

    return jax.shard_map(per_device, mesh=mesh, in_specs=in_specs, out_specs=P(("sp", "tp"), None), check_vma=False)
```

```python
import functools

import jax
import jax.numpy as jnp
from jax import lax
from jax.experimental import pallas as pl
from jax.experimental.pallas import tpu as pltpu
from jax.sharding import PartitionSpec as P

residual_scale = 8.0**0.25
branch_scale = 0.8
norm_epsilon = 1e-05
masked_score = -1e30
log2_e = 1.4426950408889634
MESH = pl.DeviceIdType.MESH


def layer_norm(values, gains):
    centered = values - jnp.mean(values, axis=-1, keepdims=True)
    variance = jnp.mean(centered * centered, axis=-1, keepdims=True)
    return centered * lax.rsqrt(variance + norm_epsilon) * gains


def fold_lanes(values, op):
    result = values[:, :128]
    for start in range(128, values.shape[1], 128):
        result = op(result, values[:, start : start + 128])
    return result


class Plan:
    def __init__(self, n, m, small, large, tokens, rows, small_size, large_size, features, units):
        self.n, self.m, self.chips, self.peers = n, m, m // 2, m
        self.slots = small + large
        self.group = n // self.slots
        half = small // 2
        self.kinds = [("s", i) for i in range(half)]
        self.kinds += [("l", i) for i in range(large)]
        self.kinds += [("s", i) for i in range(half, small)]
        self.keys = [1 if kind == "s" else 2 for kind, _ in self.kinds]
        self.natural = [self.kinds.index(("s", i)) for i in range(small)]
        self.natural += [self.kinds.index(("l", i)) for i in range(large)]
        self.tokens, self.rows, self.features = tokens, rows, features
        self.small_size, self.large_size = small_size, large_size
        tiles = units // 128
        first = (tiles + 1) // 2 * 128
        self.sizes, self.offsets = (units - first, first), (0, units - first)
        self.half_of = [(i + 1) // 2 % 2 for i in range(self.slots)]
        self.depth = features // n
        self.halves = max(1, self.depth // 128)
        self.span = self.depth // self.halves
        self.columns = [(start, tuple(max(0, min(256, size - start)) for size in self.sizes))
                        for start in range(0, first, 256)]
        self.pieces = [(tensor, j) for j in range(len(self.columns)) for tensor in (0, 1)]
        self.ups = len(self.pieces)
        self.pieces += [(2, (h, part)) for h in range(self.halves) for part in range(2)]
        keys = n * tokens
        self.high = tokens
        while self.high > 128 and self.high * keys > 2**21:
            self.high //= 2


def layer_kernel(plan, lam_small, lam_large, k_small_in, v_small_in, q_small_in, k_large_in, v_large_in,
                 q_large_in, gain_ref,
                 out_small, out_large, residual_ref, norm_ref, gate, up, down, out_ref,
                 k_small, v_small, q_small, k_large, v_large, q_large, kv, q, o, att, pool, peak, total, acc, w_out, w_gate, w_up, w_down, x, hidden,
                 kz_s, kz_r, vz_s, vz_r, qz_s, qz_r, kx_s, kx_r, vx_s, vx_r, loc, o_s, o_r,
                 wz_s, wz_r, wx_s, wx_r, own_w, wy_s, wy_r, wc_s, wc_r,
                 ag_s, ag_r, agc_s, agc_r, rc_s, rc_r,
                 ya_s, ya_r, zb_s, zb_r, za_s, za_r, yb_s, yb_r):
    slots, group, m, n = plan.slots, plan.group, plan.m, plan.n
    tokens, rows, chips, depth = plan.tokens, plan.rows, plan.chips, plan.depth
    features = plan.features
    s = lax.axis_index("sp")
    t = lax.axis_index("tp")
    a, b = s // group, lax.rem(s, group)
    y, c = t // 2, lax.rem(t, 2)
    parity = lax.rem(a, 2)
    partner = y * 2 + 1 - c
    aside = lax.rem(s + 1, n)
    mine = pl.ds(pl.multiple_of(s * tokens, tokens), tokens)
    large = a < 0
    for i, k in enumerate(plan.keys):
        if k == 2:
            large = jnp.logical_or(large, a == i)
    by_kind = ((1, jnp.logical_not(large)), (2, large))
    share = lax.rem((a + 1) // 2, 2)
    by_parity = ((0, share == 0), (1, share == 1))

    def remote(src, dst, send, recv, sp, tp):
        return pltpu.make_async_remote_copy(
            src_ref=src, dst_ref=dst, send_sem=send, recv_sem=recv,
            device_id={"sp": sp, "tp": tp}, device_id_type=MESH)

    def arrival(dst, recv):
        remote(dst, dst, kz_s.at[0], recv, aside, t).wait_recv()

    def block_of(i):
        return pl.ds(pl.multiple_of((i * group + b) * tokens, tokens), tokens)

    def source(i, what):
        kind, index = plan.kinds[i]
        return {"s": (k_small, v_small, q_small), "l": (k_large, v_large, q_large)}[kind][what].at[index]

    def to_slot(i, what):
        keys = pl.ds(0, plan.keys[i])
        dst = (kv.at[keys, mine], kv.at[pl.ds(2, 1), mine], q.at[keys, a])[what]
        send, recv = ((kz_s, kz_r), (vz_s, vz_r), (qz_s, qz_r))[what]
        return remote(source(i, what), dst, send.at[i], recv.at[a], i * group + b, t)

    def keep(i, what):
        keys = pl.ds(0, plan.keys[i])
        if what == 0:
            kv[keys, mine] = source(i, what)[...]
        elif what == 1:
            kv[pl.ds(2, 1), mine] = source(i, what)[...]
        else:
            q[keys, a] = source(i, what)[...]

    def by_head(values, out):
        width = out.shape[3]
        for part in range(out.shape[1]):
            piece = values[:, :, part * width : (part + 1) * width]
            out[:, part] = jnp.transpose(piece, (1, 0, 2))

    def peer(j):
        return a * group + lax.rem(b + j, group)

    def k_x(k, i, j):
        part = kv.at[pl.ds(0, k), block_of(i)]
        return remote(part, part, kx_s.at[i, j - 1], kx_r.at[i, j - 1], peer(j), t)

    def k_own(i, j):
        keys = pl.ds(0, plan.keys[i])
        return remote(source(i, 0), kv.at[keys, mine], kx_s.at[i, j - 1], kx_r.at[i, j - 1], peer(j), t)

    def v_own(i, j):
        return remote(source(i, 1), kv.at[pl.ds(2, 1), mine], vx_s.at[i, j - 1], vx_r.at[i, j - 1], peer(j), t)

    def v_x(i, j):
        part = kv.at[pl.ds(2, 1), block_of(i)]
        return remote(part, part, vx_s.at[i, j - 1], vx_r.at[i, j - 1], peer(j), t)

    pieces = len(plan.pieces)

    def piece_in(k, par):
        tensor, which = plan.pieces[k]
        if tensor < 2:
            start, widths = plan.columns[which]
            return (gate, up)[tensor].at[:, pl.ds(plan.offsets[par] + start, widths[par])]
        h, part = which
        size = plan.sizes[par] // 2
        return down.at[pl.ds(plan.offsets[par] + part * size, size), pl.ds(h * plan.span, plan.span)]

    def piece_at(k, par, block):
        tensor, which = plan.pieces[k]
        if tensor < 2:
            start, widths = plan.columns[which]
            return (w_gate, w_up)[tensor].at[
                pl.ds(pl.multiple_of(block * depth, depth), depth), pl.ds(start, widths[par])]
        h, part = which
        size = plan.sizes[par] // 2
        return w_down.at[h, pl.ds(part * size, size),
                         pl.ds(pl.multiple_of(block * plan.span, plan.span), plan.span)]

    def w_z(k, i):
        return remote(piece_in(k, plan.half_of[i]), piece_at(k, plan.half_of[i], s), wz_s.at[k, i], wz_r.at[k, a],
                      i * group + b, t)

    def w_own(k, par):
        return pltpu.make_async_copy(piece_in(k, par), piece_at(k, par, s), own_w.at[k])

    def w_x(k, par, i, j):
        part = piece_at(k, par, i * group + b)
        return remote(part, part, wx_s.at[k, i, j - 1], wx_r.at[k, i, j - 1], peer(j), t)

    def w_near(k):
        for i in range(slots):
            @pl.when(i == a + 1 - 2 * parity)
            def _():
                w_z(k, i).start()

    def w_far(k):
        for distance in range(1, slots):
            for i in range(slots):
                @pl.when(jnp.logical_and(jnp.abs(a - i) == distance, i != a + 1 - 2 * parity))
                def _():
                    w_z(k, i).start()

    def w_share(k):
        for par, when in by_parity:
            @pl.when(when)
            def _():
                w_own(k, par).wait()
                for i in range(slots):
                    @pl.when(a == i)
                    def _():
                        for j in range(1, group):
                            w_x(k, par, i, j).start()

    def w_pass(k, par, i):
        arrival(piece_at(k, par, i * group + b), wz_r.at[k, i])
        for j in range(1, group):
            w_x(k, par, i, j).start()

    def pass_near(k):
        for i in range(slots):
            @pl.when(i == a + 1 - 2 * parity)
            def _():
                w_pass(k, plan.half_of[i ^ 1], i)

    def pass_far(k):
        for par, when in by_parity:
            @pl.when(when)
            def _():
                for distance in range(1, slots):
                    for i in range(slots):
                        @pl.when(jnp.logical_and(jnp.abs(a - i) == distance, i != a + 1 - 2 * parity))
                        def _():
                            w_pass(k, par, i)

    def w_forward(k):
        pass_near(k)
        pass_far(k)

    def w_wait(k):
        for par, when in by_parity:
            @pl.when(when)
            def _():
                for i in range(slots):
                    for j in range(1, group):
                        block = i * group + lax.rem(b + group - j, group)
                        arrival(piece_at(k, par, block), wx_r.at[k, i, j - 1])

    def tp_of(dy):
        return lax.rem(y + dy, chips) * 2 + c

    cut = out_small.shape[0]
    deep = cut + out_large.shape[0]
    spans = ((out_small, 0, cut), (out_large, cut, out_large.shape[0]))

    def wo_at(tp, e):
        return w_out.at[pl.ds(pl.multiple_of(tp * deep + spans[e][1], 128), spans[e][2])]

    def stash(which, h, r, start, size):
        low = features // plan.halves
        return w_out.at[pl.ds((which * m + r) * rows, rows), pl.ds(h * low + start, size)]


    def wo_y(dy, e):
        part = spans[e][0]
        return remote(part, wo_at(t, e), wy_s.at[dy - 1, e], wy_r.at[chips - dy - 1, e], s, tp_of(dy))

    def wo_c(dy, e):
        part = spans[e][0]
        there = wo_at(tp_of(dy), e)
        return remote(part if dy == 0 else there, there, wc_s.at[dy, e], wc_r.at[dy, e], s, partner)

    def wo_own(e):
        return pltpu.make_async_copy(spans[e][0], wo_at(t, e), loc.at[e])

    pair = (a + 1 - 2 * parity) * group + b

    def row_z():
        return remote(x.at[0, 0], x.at[chips, 0], ag_s.at[0], ag_r.at[chips], pair, t)

    def row_y(dz, dy):
        r = dz * chips + dy
        into = dz * chips + chips - dy
        return remote(x.at[dz * chips, 0], x.at[into, 0], ag_s.at[r], ag_r.at[into], s, tp_of(dy))

    def row_near(r):
        return remote(x.at[r, 0], x.at[r, 1], agc_s.at[r], agc_r.at[r], s, partner)

    side = features // plan.halves // 2

    def half_near(h, r):
        return remote(stash(0, h, r, 0, 2 * side), stash(1, h, r, 0, 2 * side), rc_s.at[h, r], rc_r.at[h, r], s, partner)

    by_y, by_z = (0, side), (side, side)

    def y_first(h, dz, dy):
        r, into = dz * chips + dy, dz * chips + chips - dy
        return remote(stash(2, h, r, *by_y), stash(3, h, into, *by_y),
                      ya_s.at[h, r], ya_r.at[h, into], s, tp_of(dy))

    def z_second(h):
        return remote(stash(2, h, chips, *by_y), stash(3, h, 0, *by_y),
                      zb_s.at[h], zb_r.at[h], pair, t)

    def z_first(h, dy):
        return remote(stash(2, h, chips + dy, *by_z), stash(3, h, chips + dy, *by_z),
                      za_s.at[h, dy], za_r.at[h, dy], pair, t)

    def y_second(h, dy):
        return remote(stash(2, h, dy, *by_z), stash(3, h, chips - dy, *by_z),
                      yb_s.at[h, dy], yb_r.at[h, chips - dy], s, tp_of(dy))

    barrier = pltpu.get_barrier_semaphore()
    for i in range(slots):
        for tt in range(m):
            @pl.when(jnp.logical_not(jnp.logical_and(i == a, tt == t)))
            def _():
                pl.semaphore_signal(barrier, inc=1, device_id={"sp": i * group + b, "tp": tt},
                                    device_id_type=MESH)
    for j in range(1, group):
        pl.semaphore_signal(barrier, inc=1, device_id={"sp": peer(j), "tp": t}, device_id_type=MESH)
    by_head(k_large_in, k_large)
    by_head(k_small_in, k_small)
    for e in range(2):
        wo_own(e).start()
    for par, when in by_parity:
        @pl.when(when)
        def _():
            for k in range(pieces):
                w_own(k, par).start()
    by_head(v_large_in, v_large)
    by_head(v_small_in, v_small)
    pl.semaphore_wait(barrier, slots * m - 1 + group - 1)

    for what in range(3):
        for distance in range(1, slots):
            for i in range(slots):
                @pl.when(jnp.abs(a - i) == distance)
                def _():
                    to_slot(i, what).start()
        if what == 1:
            by_head(q_large_in, q_large)
            by_head(q_small_in, q_small)
    for e in range(2):
        for dy in range(1, chips):
            wo_y(dy, e).start()
        wo_c(0, e).start()
    spare_units = plan.sizes[1] - plan.sizes[0]
    if spare_units:
        @pl.when(share == 0)
        def _():
            spare = pl.ds(plan.sizes[0], spare_units)
            w_gate[:, spare] = jnp.zeros((features, spare_units), w_gate.dtype)
            w_up[:, spare] = jnp.zeros((features, spare_units), w_up.dtype)
            for h in range(plan.halves):
                w_down[h, spare, :] = jnp.zeros((spare_units, features // plan.halves), w_down.dtype)

    for i in range(slots):
        @pl.when(a == i)
        def _():
            for what in range(3):
                keep(i, what)
            for j in range(1, group):
                k_own(i, j).start()
                v_own(i, j).start()

    for distance in range(1, slots):
        for i in range(slots):
            for k, when in by_kind:
                @pl.when(jnp.logical_and(when, jnp.abs(a - i) == distance))
                def _():
                    arrival(kv.at[pl.ds(0, k), block_of(i)], kz_r.at[i])
                    for j in range(1, group):
                        k_x(k, i, j).start()
    for distance in range(1, slots):
        for i in range(slots):
            @pl.when(jnp.abs(a - i) == distance)
            def _():
                arrival(kv.at[pl.ds(2, 1), block_of(i)], vz_r.at[i])
                for j in range(1, group):
                    v_x(i, j).start()

    w_near(0)
    w_far(0)
    for k in range(pieces):
        w_share(k)

    def ready(i):
        for k, when in by_kind:
            @pl.when(when)
            def _():
                @pl.when(a != i)
                def _():
                    arrival(q.at[pl.ds(0, k), i], qz_r.at[i])

                for j in range(1, group):
                    block = i * group + lax.rem(b + group - j, group)
                    from_peer = pl.ds(pl.multiple_of(block * tokens, tokens), tokens)
                    arrival(kv.at[pl.ds(0, k), from_peer], kx_r.at[i, j - 1])
                    arrival(kv.at[pl.ds(2, 1), from_peer], vx_r.at[i, j - 1])

        @pl.when(jnp.logical_not(large))
        def _():
            both = q[0, i]
            lane = lax.broadcasted_iota(jnp.int32, both.shape, 1)
            q[1, i] = jnp.where(lane >= plan.small_size, both, jnp.zeros_like(both))
            q[0, i] = jnp.where(lane < plan.small_size, both, jnp.zeros_like(both))

    lift = large.astype(jnp.int32)
    factor = jnp.where(large, plan.large_size**-0.5 * log2_e, plan.small_size**-0.5 * log2_e)
    lam = jnp.float32(0.0)
    for i, (kind, index) in enumerate(plan.kinds):
        lam = jnp.where(a == i, (lam_small if kind == "s" else lam_large)[index], lam)
    last = (((1,), (1,)), ((), ()))
    high = plan.high
    parts = tokens // high
    wide = group * tokens
    strip = min(512, tokens)
    head = t * slots + a

    def o_copy(i, which):
        return remote(o.at[i, pl.ds(pl.multiple_of(which * rows, rows), rows)], att.at[head],
                      o_s.at[i, which], o_r.at[head], i * group + b, which)

    def attend(i, part):
        row0 = part * high
        here = pl.ds(pl.multiple_of(row0, high), high)
        queries = (q[0, i, here], q[1, i, here])

        def find(chunk, last_one):
            for which in range(2):
                for off in range(0, wide, strip):
                    at = pl.ds(pl.multiple_of(chunk * wide + off, strip), strip)
                    score = lax.dot_general(
                        queries[which], kv[which * lift, at], last, preferred_element_type=jnp.float32)
                    if last_one:
                        row = b * tokens + row0 + lax.broadcasted_iota(jnp.int32, score.shape, 0)
                        column = off + lax.broadcasted_iota(jnp.int32, score.shape, 1)
                        score = jnp.where(column <= row, score, masked_score)
                    pool[which, :, at] = score
                    top = fold_lanes(score, jnp.maximum)
                    fresh = last_one and off == 0
                    peak[which] = top if fresh else jnp.maximum(peak[which], top)

        find(i, True)
        lax.fori_loop(0, i, lambda chunk, carry: find(chunk, False) or carry, 0)
        for which in range(2):
            peak[which] = jnp.broadcast_to(
                jnp.max(peak[which], axis=1, keepdims=True), (high, 128))

        def weigh(chunk, fresh):
            for which in range(2):
                sums = outs = None
                for off in range(0, wide, strip):
                    at = pl.ds(pl.multiple_of(chunk * wide + off, strip), strip)
                    score = pool[which, :, at]
                    top = peak[which]
                    weights = jnp.concatenate(
                        [jnp.exp2((score[:, u : u + 128] - top) * factor) for u in range(0, strip, 128)],
                        axis=1)
                    part_sum = fold_lanes(weights, jnp.add)
                    part_out = jnp.dot(
                        weights.astype(jnp.bfloat16), kv[2, at], preferred_element_type=jnp.float32)
                    sums = part_sum if sums is None else sums + part_sum
                    outs = part_out if outs is None else outs + part_out
                if fresh:
                    total[which], acc[which] = sums, outs
                else:
                    total[which] += sums
                    acc[which] += outs

        weigh(i, True)
        lax.fori_loop(0, i, lambda chunk, carry: weigh(chunk, False) or carry, 0)
        outs = [acc[which] / jnp.sum(total[which], axis=1, keepdims=True) for which in range(2)]
        combined = outs[0] - lam * outs[1]
        mean_square = jnp.mean(combined * combined, axis=1, keepdims=True)
        normed = combined * lax.rsqrt(mean_square + norm_epsilon) * gain_ref[...] * branch_scale
        o[i, here] = normed.astype(o.dtype)

    def send(i):
        for which in range(tokens // rows):
            @pl.when(jnp.logical_not(jnp.logical_and(i == a, which == t)))
            def _():
                o_copy(i, which).start()

    def wo_forward():
        for dy in range(1, chips):
            for e in range(2):
                arrival(wo_at(tp_of(dy), e), wy_r.at[dy - 1, e])
                wo_c(dy, e).start()

    def step_body(i, carry):
        for at in range(slots):
            @pl.when(i == at)
            def _():
                ready(at)
                if at == slots // 2 - 1:
                    for k in (1, 2):
                        w_near(k)
                        w_far(k)
                if at == slots // 2:
                    for k in (3, 4):
                        w_near(k)
        lax.fori_loop(0, parts, lambda part, c: attend(i, part) or c, 0)

        @pl.when(i > 0)
        def _():
            send(i - 1)

        return carry

    lax.fori_loop(0, slots, step_body, 0)
    att[head] = o[a, pl.ds(pl.multiple_of(t * rows, rows), rows)]
    send(slots - 1)
    w_far(3)
    for k in range(5, pieces):
        w_near(k)
    w_far(4)
    w_forward(0)
    wo_forward()
    w_forward(1)

    for e in range(2):
        wo_own(e).wait()
        for dy in range(chips):
            block = lax.rem(y + dy, chips) * 2 + 1 - c
            arrival(wo_at(block, e), wc_r.at[dy, e])
    for h in range(m * slots):
        @pl.when(head != h)
        def _():
            arrival(att.at[h], o_r.at[h])
    for e in range(2):
        for dy in range(chips):
            wo_c(dy, e).wait_send()
    stretch = 512
    base = plan.features
    for start in range(0, features, stretch):
        cols = pl.ds(start, stretch)
        sums = None
        for tt in range(m):
            left = jnp.concatenate([att[tt * slots + i] for i in plan.natural], axis=1)
            term = jnp.dot(left, w_out[pl.ds(tt * deep, deep), cols], preferred_element_type=jnp.float32)
            sums = term if sums is None else sums + term
        pool[1, pl.ds(0, rows), pl.ds(base + start, stretch)] = (
            residual_scale * residual_ref[:, cols].astype(jnp.float32) + sums)
    x[0, 0] = layer_norm(pool[1, pl.ds(0, rows), pl.ds(base, features)], norm_ref[...]).astype(x.dtype)
    peers = plan.peers
    row_z().start()
    for dy in range(1, chips):
        row_y(0, dy).start()
    row_near(0).start()
    for k in range(5, pieces):
        w_far(k)

    def gate_up(j, lo, hi):
        start, widths = plan.columns[j]
        cols = pl.ds(start, max(widths))

        def one(r, carry):
            both = x[r].reshape(2 * rows, features)
            g = jnp.dot(both, w_gate[:, cols], preferred_element_type=jnp.float32)
            u = jnp.dot(both, w_up[:, cols], preferred_element_type=jnp.float32)
            hidden[r, :, cols] = (g / (1.0 + jnp.exp(-g)) * u).astype(hidden.dtype)
            return carry

        lax.fori_loop(lo, hi, one, 0)

    def forward_to(last):
        for k in range(state["done"], min(last, pieces)):
            if k < 3:
                pass_near(k)
            pass_far(k)
            state["done"] = k + 1

    def rows_y(dz):
        for dy in range(1, chips):
            r = dz * chips + dy
            arrival(x.at[r, 0], ag_r.at[r])
            row_near(r).start()

    def rows_near(dz):
        for r in range(dz * chips, dz * chips + chips):
            arrival(x.at[r, 1], agc_r.at[r])

    def columns_here(j):
        w_wait(2 * j)
        w_wait(2 * j + 1)

    state = {"done": 2}
    ups = plan.ups
    early = len(plan.columns) - 1
    forward_to(3)
    for k in range(3, pieces):
        pass_near(k)
    forward_to(4)
    rows_y(0)
    forward_to(5)
    arrival(x.at[chips, 0], ag_r.at[chips])
    for dy in range(1, chips):
        row_y(1, dy).start()
    row_near(chips).start()
    for i in range(slots):
        @pl.when(a != i)
        def _():
            for what in range(3):
                to_slot(i, what).wait_send()

        for kind, when in by_kind:
            @pl.when(when)
            def _():
                for j in range(1, group):
                    k_x(kind, i, j).wait_send()
                    v_x(i, j).wait_send()
        for which in range(tokens // rows):
            @pl.when(jnp.logical_not(jnp.logical_and(i == a, which == t)))
            def _():
                o_copy(i, which).wait_send()
    for e in range(2):
        for dy in range(1, chips):
            wo_y(dy, e).wait_send()
    rows_near(0)
    for j in range(early):
        forward_to(2 * j + 2)
        columns_here(j)
        gate_up(j, 0, chips)
    forward_to(ups)
    rows_y(1)
    forward_to(ups + 1)
    rows_near(1)
    gate_up(0, chips, peers)
    forward_to(ups + 2)
    if early > 1:
        gate_up(1, chips, peers)
    forward_to(ups + 3)
    for j in range(2, early):
        gate_up(j, chips, peers)
    columns_here(early)
    gate_up(early, 0, peers)
    forward_to(ups + 4)

    low = features // plan.halves
    band = min(512, low)
    per_plane = high // rows

    def kept(r, cols):
        return pool.at[r // per_plane, pl.ds(r % per_plane * rows, rows), cols]

    def down_rows(h, r):
        for start in range(0, low, band):
            cols = pl.ds(start, band)
            part = jnp.dot(hidden[r], w_down[h, :, cols], preferred_element_type=jnp.float32)
            kept(r, pl.ds(h * low + start, band))[...] = part[:rows]
            stash(0, h, r, start, band)[...] = part[rows:].astype(w_out.dtype)

    def chip_sum(h, r, which):
        cols = pl.ds(h * low + which * side, side)
        return kept(r, cols)[...] + stash(1, h, r, which * side, side)[...].astype(jnp.float32)

    def down_half(h):
        order = [chips + dy for dy in range(1, chips)] + [chips] + list(range(1, chips)) + [0]

        def pass_on(r):
            dz, dy = r // chips, r % chips
            arrival(stash(1, h, r, 0, 2 * side), rc_r.at[h, r])
            if dy:
                stash(2, h, r, *by_y)[...] = chip_sum(h, r, 0).astype(w_out.dtype)
                y_first(h, dz, dy).start()
            if dz:
                stash(2, h, r, *by_z)[...] = chip_sum(h, r, 1).astype(w_out.dtype)
                z_first(h, dy).start()

        for place, r in enumerate(order):
            down_rows(h, r)
            half_near(h, r).start()
            if place:
                pass_on(order[place - 1])
        pass_on(0)

    def plane_sum(h, dz):
        result = chip_sum(h, dz * chips, 0)
        for dy in range(1, chips):
            r = dz * chips + dy
            arrival(stash(3, h, r, *by_y), ya_r.at[h, r])
            result += stash(3, h, r, *by_y)[...].astype(jnp.float32)
        return result

    def line_sum(h, dy):
        arrival(stash(3, h, chips + dy, *by_z), za_r.at[h, dy])
        return chip_sum(h, dy, 1) + stash(3, h, chips + dy, *by_z)[...].astype(jnp.float32)

    def second_sums(h):
        stash(2, h, chips, *by_y)[...] = plane_sum(h, 1).astype(w_out.dtype)
        z_second(h).start()
        for dy in range(1, chips):
            stash(2, h, dy, *by_z)[...] = line_sum(h, dy).astype(w_out.dtype)
            y_second(h, dy).start()

    def finish(h):
        first = plane_sum(h, 0)
        arrival(stash(3, h, 0, *by_y), zb_r.at[h])
        first += stash(3, h, 0, *by_y)[...].astype(jnp.float32)
        second = line_sum(h, 0)
        for dy in range(1, chips):
            arrival(stash(3, h, dy, *by_z), yb_r.at[h, dy])
            second += stash(3, h, dy, *by_z)[...].astype(jnp.float32)
        result = jnp.concatenate([first, second], axis=1)
        for block in range(n):
            cols = pl.ds(block * depth + h * plan.span, plan.span)
            out_ref[:, cols] = (
                residual_scale * x[0, 0, :, cols].astype(jnp.float32)
                + 0.5 * result[:, block * plan.span : (block + 1) * plan.span]
            ).astype(out_ref.dtype)

    for h in range(plan.halves):
        first = plan.ups + 2 * h
        forward_to(first + 2)
        w_wait(first)
        w_wait(first + 1)
        down_half(h)
        if h:
            second_sums(h - 1)
    second_sums(plan.halves - 1)
    for i in range(slots):
        @pl.when(a != i)
        def _():
            for k in range(pieces):
                w_z(k, i).wait_send()

        for par, when in by_parity:
            @pl.when(when)
            def _():
                for j in range(1, group):
                    for k in range(pieces):
                        w_x(k, par, i, j).wait_send()
    for h in range(plan.halves):
        finish(h)

    row_z().wait_send()
    for r in range(peers):
        row_near(r).wait_send()
        for h in range(plan.halves):
            half_near(h, r).wait_send()
            if r % chips:
                y_first(h, r // chips, r % chips).wait_send()
        if r % chips:
            row_y(r // chips, r % chips).wait_send()
    for h in range(plan.halves):
        z_second(h).wait_send()
        for dy in range(chips):
            z_first(h, dy).wait_send()
            if dy:
                y_second(h, dy).wait_send()


def run_layer(plan, lams, small, large, gain, outs, residual, norm_gain, mixer, width):
    dma = pltpu.SemaphoreType.DMA
    slots, n, m, peers, chips = plan.slots, plan.n, plan.m, plan.peers, plan.chips
    rows, features, units, halves = plan.rows, plan.features, plan.sizes[1], plan.halves
    high, pieces = plan.high, len(plan.pieces)
    anywhere = pl.BlockSpec(memory_space=pl.ANY)
    vmem = pl.BlockSpec(memory_space=pltpu.VMEM)
    smem = pl.BlockSpec(memory_space=pltpu.SMEM)
    others, ahead = max(plan.group - 1, 1), max(chips - 1, 1)
    bf16, f32 = jnp.bfloat16, jnp.float32
    return pl.pallas_call(
        functools.partial(layer_kernel, plan),
        out_shape=jax.ShapeDtypeStruct((rows, features), bf16),
        in_specs=[smem] * 2 + [vmem] * 7 + [anywhere] * 2 + [vmem] * 2 + [anywhere] * 3,
        out_specs=vmem,
        scratch_shapes=[
            pltpu.VMEM((small[0].shape[1], 1, plan.tokens, width), bf16),
            pltpu.VMEM((small[0].shape[1], 1, plan.tokens, width), bf16),
            pltpu.VMEM((small[0].shape[1], 1, plan.tokens, width), bf16),
            pltpu.VMEM((large[0].shape[1], 2, plan.tokens, width), bf16),
            pltpu.VMEM((large[0].shape[1], 1, plan.tokens, width), bf16),
            pltpu.VMEM((large[0].shape[1], 2, plan.tokens, width), bf16),
            pltpu.VMEM((3, n * plan.tokens, width), bf16),
            pltpu.VMEM((2, slots, plan.tokens, width), bf16),
            pltpu.VMEM((slots, plan.tokens, width), bf16),
            pltpu.VMEM((m * slots, rows, width), bf16),
            pltpu.VMEM((2, high, n * plan.tokens), f32),
            pltpu.VMEM((2, high, 128), f32),
            pltpu.VMEM((2, high, 128), f32),
            pltpu.VMEM((2, high, width), f32),
            pltpu.VMEM((max(m * slots * width, 4 * m * rows), features), bf16),
            pltpu.VMEM((features, units), bf16),
            pltpu.VMEM((features, units), bf16),
            pltpu.VMEM((halves, units, features // halves), bf16),
            pltpu.VMEM((peers, 2, rows, features), bf16),
            pltpu.VMEM((peers, 2 * rows, units), bf16),
            dma((slots,)), dma((slots,)), dma((slots,)), dma((slots,)), dma((slots,)), dma((slots,)),
            dma((slots, others)), dma((slots, others)), dma((slots, others)), dma((slots, others)),
            dma((2,)),
            dma((slots, plan.tokens // rows)), dma((m * slots,)),
            dma((pieces, slots)), dma((pieces, slots)),
            dma((pieces, slots, others)), dma((pieces, slots, others)),
            dma((pieces,)),
            dma((ahead, 2)), dma((ahead, 2)), dma((chips, 2)), dma((chips, 2)),
            dma((peers,)), dma((peers,)), dma((peers,)), dma((peers,)),
            dma((halves, peers)), dma((halves, peers)),
            dma((halves, peers)), dma((halves, peers)), dma((halves,)), dma((halves,)),
            dma((halves, chips)), dma((halves, chips)), dma((halves, chips)), dma((halves, chips)),
        ],
        compiler_params=pltpu.CompilerParams(
            vmem_limit_bytes=61 * 2**20, has_side_effects=True, collective_id=0),
        cost_estimate=pl.CostEstimate(
            flops=60_000_000_000, bytes_accessed=16_000_000, transcendentals=8_000_000),
        name="layer",
    )(*lams, *small, *large, gain.reshape(1, width), *outs, residual, norm_gain.reshape(1, features), *mixer)


def per_device(
    residual, query_small, key_small, value_small, query_large, key_large, value_large,
    lambda_small, lambda_large, head_gain, output_small, output_large, norm_gain,
    gate_weight, up_weight, down_weight,
):
    tokens, heads_small, width = value_small.shape
    heads_large = value_large.shape[1]
    rows, features = residual.shape
    n, m = lax.axis_size("sp"), lax.axis_size("tp")
    short = -gate_weight.shape[1] % 128
    if short:
        gate_weight = jnp.pad(gate_weight, ((0, 0), (0, short)))
        up_weight = jnp.pad(up_weight, ((0, 0), (0, short)))
        down_weight = jnp.pad(down_weight, ((0, short), (0, 0)))
    plan = Plan(n, m, heads_small, heads_large, tokens, rows, query_small.shape[2] // 2,
                query_large.shape[2] // 2, features, gate_weight.shape[1])

    small = (key_small, value_small, query_small)
    large = (key_large, value_large, query_large)
    return run_layer(
        plan, (lambda_small, lambda_large), small, large, head_gain, (output_small, output_large),
        residual, norm_gain, (gate_weight, up_weight, down_weight), width)


def solution(mesh):
    in_specs = (
        P(("sp", "tp"), None), P("sp", "tp", None), P("sp", "tp", None), P("sp", "tp", None),
        P("sp", "tp", None), P("sp", "tp", None), P("sp", "tp", None), P("tp"), P("tp"), P(),
        P("tp", None), P("tp", None), P(), P("sp", "tp"), P("sp", "tp"), P("tp", "sp"),
    )

    return jax.shard_map(per_device, mesh=mesh, in_specs=in_specs, out_specs=P(("sp", "tp"), None), check_vma=False)
```
